512 devices in a mesh: ep: 128 (over z, y, core), tp: 4 (over x).
Axes of the slice: x: 4, y: 8, z: 8, core: 2. Of those that a mesh axis runs over, the one named last changes fastest.
Arguments:
- hidden_in: bfloat16 [2048, 1024], P('ep'), may hold values from -6 to 6
- prior_state: float32 [2048, 8, 128, 128], P('ep', 'tp'), may hold values from -4 to 4
- mix_gain: float32 [1024], replicated, may hold values from 0.1 to 1.9
- query_w: bfloat16 [1024, 1024], P(None, 'tp'), may hold values from -0.1875 to 0.1875
- key_w: bfloat16 [1024, 1024], P(None, 'tp'), may hold values from -0.1875 to 0.1875
- value_w: bfloat16 [1024, 1024], P(None, 'tp'), may hold values from -0.1875 to 0.1875
- decay_w: bfloat16 [1024, 8], P(None, 'tp'), may hold values from -0.1875 to 0.1875
- beta_w: bfloat16 [1024, 8], P(None, 'tp'), may hold values from -0.1875 to 0.1875
- decay_rate: float32 [8], P('tp'), may hold values from 0.05 to 3
- head_gain: float32 [128], replicated, may hold values from 0.1 to 1.9
- out_w: bfloat16 [1024, 1024], P('tp'), may hold values from -0.1875 to 0.1875
- ffn_gain: float32 [1024], replicated, may hold values from 0.1 to 1.9
- expert_ids: int32 [2048, 2], P('ep'), may hold values from 0 to 127, all different within a row; in each aligned block of 16 rows (0 to 15, 16 to 31, ...) at most 2 rows name the same one
- group_share: float32 [2048], P('ep'), may hold values from 0.3 to 1
- expert_share: float32 [2048, 2], P('ep'), may hold values from 0.1 to 1
- expert_gate: bfloat16 [128, 1024, 512], P('ep', None, 'tp'), may hold values from -0.1875 to 0.1875
- expert_up: bfloat16 [128, 1024, 512], P('ep', None, 'tp'), may hold values from -0.1875 to 0.1875
- expert_down: bfloat16 [128, 512, 1024], P('ep', 'tp'), may hold values from -0.25 to 0.25
- dense_gate: bfloat16 [4096, 1024], P('ep', 'tp'), may hold values from -0.1875 to 0.1875
- dense_up: bfloat16 [4096, 1024], P('ep', 'tp'), may hold values from -0.1875 to 0.1875
- dense_down: bfloat16 [4096, 1024], P('ep', 'tp'), may hold values from -0.25 to 0.25
- branch_gate: bfloat16 [1024], replicated, may hold values from -0.1875 to 0.1875
Outputs:
- layer_out: bfloat16 [2048, 1024], P('ep', 'tp')
The draws below stay inside these ranges and needn't reach their ends.
Inputs may be any that keep to these rules, and one draw needn't show every extreme that they name: `expert_ids`: each row names 2 different experts. Among the rows of one device, no expert is named by more than 2 rows, and in every draw some expert is named by exactly 2 rows of some device.
All inputs are finite; a program needn't handle non-finite values.
Results may differ from the reference program's by a relative error of at most 0.02.
Values may be sent and summed in bfloat16 or wider, within the bound.
No kernel may reach another device: no remote copies, remote signals or barrier semaphores. Data moves between devices by JAX's collectives and lax.ppermute only.
A program may use at most 64 MiB of HBM per device.

```python
import math
import jax
import jax.numpy as jnp
import numpy as np
from jax import lax

D = 1024
HEADS = 8
DK = 128
DV = 128
FF = 512
FD = 4096
TOPK = 2
SEQ_DEV = 16
SEQS = 2048
EXPERTS = 128
CAP = 2
N_EP = 128
N_TP = 4


def levels(own_key, extent, split, least, largest):
    loudness = 1.0
    for axis_at, shards_of in split:
        heights = jax.random.uniform(jax.random.fold_in(jax.random.fold_in(own_key, 6), axis_at), (shards_of,), jnp.float32, least / len(split), largest / len(split))
        loudness = loudness * jnp.repeat(jnp.exp(heights), extent[axis_at] // shards_of).reshape((-1,) + (1,) * (len(extent) - 1 - axis_at))
    return loudness


def assign_block(stream_key, own, number, rows, count, top, bound, skew):
    order = jax.random.permutation(stream_key, count)
    crowded, usual = shares(count, rows * top, bound, skew, True), shares(count, rows * top, bound, skew, False)
    places = jnp.arange(count)

    def named(tallies, rotation):
        used = int((tallies > 0).sum())
        fixed = max(1, used // 4)
        shifted = fixed + (places - fixed + rotation * (used - fixed)) % max(1, count - fixed)
        return jnp.zeros((count,), jnp.int32).at[order[jnp.where(places < fixed, places, shifted)]].set(jnp.asarray(tallies, jnp.int32))

    tallies = jnp.where(number % 4 == 0, named(crowded, number // 4), named(usual, number - number // 4 - 1))
    mixed = jax.random.permutation(jax.random.fold_in(own, 3), count)
    donor, receiver = mixed[0:count // 2 * 2:2], mixed[1:count // 2 * 2:2]
    room = jnp.minimum(tallies[donor] - 1, bound - tallies[receiver]) // 2
    room = jnp.where((donor == order[0]) | (receiver == order[0]) | (tallies[receiver] == 0), 0, jnp.maximum(room, 0))
    shifted = jax.random.randint(jax.random.fold_in(own, 4), (count // 2,), 0, 1 << 20) % (room + 1)
    tallies = tallies.at[donor].add(-shifted).at[receiver].add(shifted)
    labels = jnp.searchsorted(jnp.cumsum(tallies), jnp.arange(rows * top), side="right").astype(jnp.int32)
    listing = labels.reshape(top, rows).T
    listing = listing[jax.random.permutation(jax.random.fold_in(own, 1), rows)]
    rotation = jax.random.randint(jax.random.fold_in(own, 2), (rows, 1), 0, top)
    return jnp.take_along_axis(listing, (jnp.arange(top)[None, :] + rotation) % top, axis=1)


def shares(count, total, reach, skew, full):
    loads = [(1 << 20) // math.isqrt(grade ** skew) + 1 for grade in range(1, count + 1)]
    largest = reach if full else min(reach, max(-(-total // count), total * loads[0] // sum(loads)))
    least = 1 if total - largest >= count - 1 else 0
    counts, surplus = [largest] + [least] * (count - 1), total - largest - least * (count - 1)
    while surplus > 0:
        movable = [i for i in range(1, count) if counts[i] < largest] or [i for i in range(1, count) if counts[i] < reach]
        mass, left = sum([loads[i] for i in movable]), surplus
        for i in movable:
            extra = min(reach - counts[i], max(1, left * loads[i] // mass), surplus)
            counts[i] = counts[i] + extra
            surplus = surplus - extra
    return np.array(counts)


def normal_values(stream_key, shape, scale, reach, cuts=(), kind=jnp.bfloat16):
    values = jax.random.normal(stream_key, shape, jnp.float32) * scale
    if len(cuts) > 0:
        values = levels(stream_key, shape, cuts, -0.22, 0.18) * values
    return jnp.clip(values, min=-reach, max=reach).astype(kind)


def setup_inputs(seed: int = 0) -> dict:
    arg_keys = jax.random.split(jax.random.key(seed), 23)
    hidden_in = normal_values(arg_keys[0], (SEQS, D), 1.0, 6.0, ((0, 128),))
    prior_state = normal_values(arg_keys[1], (SEQS, HEADS, DK, DV), 0.3, 4.0, ((0, 128), (1, 4)), jnp.float32)
    mix_gain = jnp.clip(1.0 + 0.18 * jax.random.normal(arg_keys[2], (D,), jnp.float32), 0.1, 1.9)
    query_w = normal_values(arg_keys[3], (D, HEADS * DK), D ** -0.5, 0.1875, ((1, 4),))
    key_w = normal_values(arg_keys[4], (D, HEADS * DK), D ** -0.5, 0.1875, ((1, 4),))
    value_w = normal_values(arg_keys[5], (D, HEADS * DV), D ** -0.5, 0.1875, ((1, 4),))
    decay_w = normal_values(arg_keys[6], (D, HEADS), D ** -0.5, 0.1875, ((1, 4),))
    beta_w = normal_values(arg_keys[7], (D, HEADS), D ** -0.5, 0.1875, ((1, 4),))
    decay_rate = jnp.clip(jnp.exp(math.log(3.0) - 4.0943445 * jax.random.uniform(arg_keys[8], (HEADS,), jnp.float32) ** levels(arg_keys[8], (HEADS,), ((0, 4),), -0.2, 0.2)), 0.05, 3.0)
    head_gain = jnp.clip(1.0 + 0.18 * jax.random.normal(arg_keys[9], (DV,), jnp.float32), 0.1, 1.9)
    out_w = normal_values(arg_keys[10], (HEADS * DV, D), (HEADS * DV) ** -0.5, 0.1875, ((0, 4),))
    ffn_gain = jnp.clip(1.0 + 0.18 * jax.random.normal(arg_keys[11], (D,), jnp.float32), 0.1, 1.9)
    expert_ids_keys = jax.random.split(jax.random.fold_in(arg_keys[12], 1), SEQS // SEQ_DEV)
    expert_ids_turns = jax.random.permutation(jax.random.fold_in(arg_keys[12], 3), SEQS // SEQ_DEV)
    expert_ids = jax.vmap(lambda own, number: assign_block(jax.random.fold_in(arg_keys[12], 2), own, number, SEQ_DEV, EXPERTS, TOPK, CAP, 2))(expert_ids_keys, expert_ids_turns).reshape((SEQS, TOPK))
    group_share = jnp.clip(0.3 + 0.7 * jax.random.uniform(arg_keys[13], (SEQS,), jnp.float32) ** levels(arg_keys[13], (SEQS,), ((0, 128),), -0.2, 0.2), 0.3, 1.0)
    expert_share = jnp.clip(0.1 + 0.9 * jax.random.uniform(arg_keys[14], (SEQS, TOPK), jnp.float32) ** levels(arg_keys[14], (SEQS, TOPK), ((0, 128),), -0.2, 0.2), 0.1, 1.0)
    expert_gate = normal_values(arg_keys[15], (EXPERTS, D, FF), D ** -0.5, 0.1875, ((0, 128), (2, 4)))
    expert_up = normal_values(arg_keys[16], (EXPERTS, D, FF), D ** -0.5, 0.1875, ((0, 128), (2, 4)))
    expert_down = normal_values(arg_keys[17], (EXPERTS, FF, D), FF ** -0.5, 0.25, ((0, 128), (1, 4)))
    dense_gate = normal_values(arg_keys[18], (FD, D), D ** -0.5, 0.1875, ((0, 128), (1, 4)))
    dense_up = normal_values(arg_keys[19], (FD, D), D ** -0.5, 0.1875, ((0, 128), (1, 4)))
    dense_down = normal_values(arg_keys[20], (FD, D), (FD // 8) ** -0.5, 0.25, ((0, 128), (1, 4)))
    branch_gate = normal_values(arg_keys[21], (D,), D ** -0.5, 0.1875)
    return {"hidden_in": hidden_in, "prior_state": prior_state, "mix_gain": mix_gain, "query_w": query_w, "key_w": key_w, "value_w": value_w, "decay_w": decay_w, "beta_w": beta_w, "decay_rate": decay_rate, "head_gain": head_gain, "out_w": out_w, "ffn_gain": ffn_gain, "expert_ids": expert_ids, "group_share": group_share, "expert_share": expert_share, "expert_gate": expert_gate, "expert_up": expert_up, "expert_down": expert_down, "dense_gate": dense_gate, "dense_up": dense_up, "dense_down": dense_down, "branch_gate": branch_gate}


def rms_scale(values, gain, floor):
    return values * lax.rsqrt(lax.optimization_barrier(jnp.mean(values * values, axis=-1, keepdims=True)) + floor) * gain

def unit_rows(values):
    return values * lax.rsqrt(lax.optimization_barrier(jnp.sum(values * values, axis=-1, keepdims=True)) + 1.0)

def delta_read(queries, key_rows, value_rows, beta_vals, decay_vals, prior_state):
    stacked = jnp.stack([queries, key_rows], axis=2)
    readout = jnp.einsum('shcd,shde->shce', stacked, prior_state, precision=lax.Precision.HIGHEST)
    intersection = lax.optimization_barrier(jnp.sum(queries * key_rows, axis=-1)) * beta_vals
    return decay_vals[..., None] * readout[:, :, 0] + intersection[..., None] * (value_rows - decay_vals[..., None] * readout[:, :, 1])

def experts_sum(normed2, expert_ids, route_weight, expert_gate, expert_up, expert_down):
    total_rows = normed2.shape[0]
    slot_total = N_EP * CAP

    def one_expert(totals, inputs):
        expert_index, w_gate, w_up, w_down = inputs
        matches = expert_ids == expert_index
        token_weight = lax.optimization_barrier(jnp.sum(jnp.where(matches, route_weight, 0.0), axis=1))
        routed = jnp.any(matches, axis=1)
        slot_rank = jnp.cumsum(routed.astype(jnp.int32)) - 1
        target = jnp.where(routed, slot_rank, slot_total).astype(jnp.int32)
        source = jnp.zeros((slot_total + 1,), jnp.int32).at[target].set(jnp.arange(total_rows, dtype=jnp.int32))[:slot_total]
        row_block = normed2[source]
        gate_pre = jnp.dot(row_block, w_gate, preferred_element_type=jnp.float32)
        up_pre = jnp.dot(row_block, w_up, preferred_element_type=jnp.float32)
        hidden = (jax.nn.silu(gate_pre) * up_pre).astype(jnp.bfloat16)
        rounded = jnp.dot(hidden, w_down, preferred_element_type=jnp.float32).astype(jnp.bfloat16)
        expert_out = lax.optimization_barrier(rounded).astype(jnp.float32)
        is_valid = jnp.arange(slot_total) < jnp.sum(routed.astype(jnp.int32))
        row_scale = jnp.where(is_valid, token_weight[source], 0.0)
        totals = totals.at[source].add(expert_out * row_scale[:, None])
        return (totals, None)
    start_sum = jnp.zeros((total_rows, normed2.shape[1]), jnp.float32)
    totals, _ = lax.scan(one_expert, start_sum, (jnp.arange(EXPERTS, dtype=jnp.int32), expert_gate, expert_up, expert_down))
    return totals

def reference(hidden_in, prior_state, mix_gain, query_w, key_w, value_w, decay_w, beta_w, decay_rate, head_gain, out_w, ffn_gain, expert_ids, group_share, expert_share, expert_gate, expert_up, expert_down, dense_gate, dense_up, dense_down, branch_gate):
    total_rows = hidden_in.shape[0]
    normed = rms_scale(hidden_in.astype(jnp.float32), mix_gain, 0.1).astype(jnp.bfloat16)
    queries = unit_rows(jnp.dot(normed, query_w, preferred_element_type=jnp.float32).reshape(total_rows, HEADS, DK))
    key_rows = unit_rows(jnp.dot(normed, key_w, preferred_element_type=jnp.float32).reshape(total_rows, HEADS, DK))
    value_rows = jnp.dot(normed, value_w, preferred_element_type=jnp.float32).reshape(total_rows, HEADS, DV)
    beta_vals = jax.nn.sigmoid(jnp.dot(normed, beta_w, preferred_element_type=jnp.float32))
    decay_vals = jnp.exp(-decay_rate * jax.nn.softplus(jnp.dot(normed, decay_w, preferred_element_type=jnp.float32)))
    readout = delta_read(queries, key_rows, value_rows, beta_vals, decay_vals, prior_state)
    head_out = rms_scale(readout, head_gain, 0.01).astype(jnp.bfloat16)
    grouped = head_out.reshape(total_rows, N_TP, HEADS * DV // N_TP).astype(jnp.float32)
    out_groups = out_w.reshape(N_TP, HEADS * DV // N_TP, D).astype(jnp.float32)
    partial_out = jnp.einsum('sgk,gkd->gsd', grouped, out_groups).astype(jnp.bfloat16)
    mix = lax.optimization_barrier(jnp.sum(partial_out.astype(jnp.float32), axis=0))
    resid = (hidden_in.astype(jnp.float32) + mix).astype(jnp.bfloat16)
    normed2 = rms_scale(resid.astype(jnp.float32), ffn_gain, 0.1).astype(jnp.bfloat16)
    route_weight = group_share[:, None] * expert_share / lax.optimization_barrier(jnp.sum(expert_share, axis=1, keepdims=True))
    moe = experts_sum(normed2, expert_ids, route_weight, expert_gate, expert_up, expert_down)
    gate_pre = jnp.dot(normed2, dense_gate.T, preferred_element_type=jnp.float32)
    up_pre = jnp.dot(normed2, dense_up.T, preferred_element_type=jnp.float32)
    branch_hidden = (jax.nn.silu(gate_pre) * up_pre).astype(jnp.bfloat16)
    branch = jnp.dot(branch_hidden, dense_down, preferred_element_type=jnp.float32)
    branch_weight = jax.nn.sigmoid(jnp.dot(normed2, branch_gate, preferred_element_type=jnp.float32))
    return (resid.astype(jnp.float32) + moe + branch_weight[:, None] * branch).astype(jnp.bfloat16)
```

```python
import jax
import jax.numpy as jnp
from jax import lax
from jax.sharding import Mesh
from jax.sharding import PartitionSpec as P

EP = ("z", "y", "c")
BF = jnp.bfloat16
F32 = jnp.float32


def rms_scale(values, gain, floor):
    return values * lax.rsqrt(jnp.mean(values * values, axis=-1, keepdims=True) + floor) * gain


def unit_rows(values):
    return values * lax.rsqrt(jnp.sum(values * values, axis=-1, keepdims=True) + 1.0)


def delta_read(queries, key_rows, value_rows, beta_vals, decay_vals, prior_state):
    stacked = jnp.stack([queries, key_rows], axis=2)
    readout = jnp.einsum("shcd,shde->shce", stacked, prior_state, precision=lax.Precision.HIGHEST)
    intersection = jnp.sum(queries * key_rows, axis=-1) * beta_vals
    return decay_vals[..., None] * readout[:, :, 0] + intersection[..., None] * (
        value_rows - decay_vals[..., None] * readout[:, :, 1]
    )


def dot32(a, b):
    return jnp.dot(a, b, preferred_element_type=F32)


def exchange(blocks, axis):
    return lax.all_to_all(blocks, axis, split_axis=0, concat_axis=0, tiled=True)


def local(
    hidden_in,
    prior_state,
    mix_gain,
    query_w,
    key_w,
    value_w,
    decay_w,
    beta_w,
    decay_rate,
    head_gain,
    out_w,
    ffn_gain,
    expert_ids,
    group_share,
    expert_share,
    expert_gate,
    expert_up,
    expert_down,
    dense_gate,
    dense_up,
    dense_down,
    branch_gate,
):
    rows, width = hidden_in.shape
    heads, dk, dv = prior_state.shape[1:]
    n_ep = lax.axis_size(EP)
    n_tp = lax.axis_size("x")
    n_z = lax.axis_size("z")
    quarter = width // n_tp
    cap = 2
    per_z = rows // n_z
    tp_at = lax.axis_index("x")
    hid = dense_gate.shape[0]

    dense_all = jnp.concatenate([dense_gate, dense_up, dense_down], axis=0)
    copies = jnp.broadcast_to(dense_all, (n_z, *dense_all.shape))
    dense_z = exchange(copies, "z").reshape(n_z, 3, hid, quarter)

    normed = rms_scale(hidden_in.astype(F32), mix_gain, 0.1).astype(BF)
    queries = unit_rows(dot32(normed, query_w).reshape(rows, heads, dk))
    key_rows = unit_rows(dot32(normed, key_w).reshape(rows, heads, dk))
    value_rows = dot32(normed, value_w).reshape(rows, heads, dv)
    beta_vals = jax.nn.sigmoid(dot32(normed, beta_w))
    decay_vals = jnp.exp(-decay_rate * jax.nn.softplus(dot32(normed, decay_w)))
    readout = delta_read(queries, key_rows, value_rows, beta_vals, decay_vals, prior_state)
    head_out = rms_scale(readout, head_gain, 0.01).astype(BF).reshape(rows, heads * dv)
    partial_out = dot32(head_out, out_w).astype(BF)
    partials = exchange(jnp.broadcast_to(partial_out, (n_tp, rows, width)), "x")
    mix = jnp.sum(partials.astype(F32), axis=0)
    resid = (hidden_in.astype(F32) + mix).astype(BF)
    normed2 = rms_scale(resid.astype(F32), ffn_gain, 0.1).astype(BF)
    own = lax.dynamic_slice_in_dim(normed2, tp_at * quarter, quarter, 1)
    resid_own = lax.dynamic_slice_in_dim(resid, tp_at * quarter, quarter, 1).astype(F32)
    branch_weight = jax.nn.sigmoid(dot32(normed2, branch_gate))
    route_weight = (
        group_share[:, None] * expert_share / jnp.sum(expert_share, axis=1, keepdims=True)
    )

    same = expert_ids[:, :, None, None] == expert_ids[None, None, :, :]
    earlier = jnp.arange(rows)[:, None] > jnp.arange(rows)[None, :]
    rank = jnp.sum(same & earlier[:, None, :, None], axis=(2, 3)).astype(jnp.int32)
    dest = jnp.arange(n_ep)[:, None, None, None]
    slot = jnp.arange(cap)[None, :, None, None]
    chosen = (expert_ids[None, None] == dest) & (rank[None, None] == slot)
    pick_expert = jnp.any(chosen, axis=3)
    dense_row = (jnp.arange(n_ep) // (n_ep // n_z))[:, None] * per_z + jnp.arange(per_z)[None, :]
    pick_dense = dense_row[:, :, None] == jnp.arange(rows)
    pick = jnp.concatenate([pick_expert, pick_dense], axis=1).astype(BF)
    block = cap + per_z
    sent = dot32(pick.reshape(n_ep * block, rows), own).astype(BF)
    arrived = exchange(sent.reshape(n_ep, block, quarter), EP)
    moe_rows = arrived[:, :cap].reshape(n_ep * cap, quarter)
    dense_rows = arrived[:, cap:].reshape(n_ep * per_z, quarter)

    n_hid = n_z * hid
    gate_z = dense_z[:, 0].reshape(n_hid, quarter)
    up_z = dense_z[:, 1].reshape(n_hid, quarter)
    down_z = dense_z[:, 2].reshape(n_hid, quarter)
    contract = (((1,), (1,)), ((), ()))
    gate_part = lax.dot_general(dense_rows, gate_z, contract, preferred_element_type=F32)
    up_part = lax.dot_general(dense_rows, up_z, contract, preferred_element_type=F32)
    share = n_hid // n_tp
    pre = jnp.stack(
        [gate_part.reshape(-1, n_tp, share), up_part.reshape(-1, n_tp, share)], axis=2
    ).astype(BF)
    pre = jnp.moveaxis(pre, 1, 0).reshape(n_tp, -1, 2 * share)
    moe_copies = jnp.broadcast_to(moe_rows, (n_tp, *moe_rows.shape))
    first = exchange(jnp.concatenate([moe_copies, pre], axis=2), "x")

    full_rows = jnp.moveaxis(first[:, :, :quarter], 0, 1).reshape(n_ep * cap, width)
    pre_sum = jnp.sum(first[:, :, quarter:].astype(F32), axis=0)
    dense_hidden = (jax.nn.silu(pre_sum[:, :share]) * pre_sum[:, share:]).astype(BF)
    gate_pre = dot32(full_rows, expert_gate[0])
    up_pre = dot32(full_rows, expert_up[0])
    hidden = (jax.nn.silu(gate_pre) * up_pre).astype(BF)
    expert_part = dot32(hidden, expert_down[0]).astype(BF)
    part_blocks = jnp.moveaxis(expert_part.reshape(n_ep * cap, n_tp, quarter), 1, 0)
    hidden_copies = jnp.broadcast_to(dense_hidden, (n_tp, *dense_hidden.shape))
    second = exchange(jnp.concatenate([part_blocks, hidden_copies], axis=2), "x")

    expert_out = jnp.sum(second[:, :, :quarter].astype(F32), axis=0).astype(BF)
    all_hidden = jnp.moveaxis(second[:, :, quarter:], 0, 1).reshape(n_ep * per_z, n_hid)
    dense_out = dot32(all_hidden, down_z).astype(BF)
    back = jnp.concatenate(
        [expert_out.reshape(n_ep, cap, quarter), dense_out.reshape(n_ep, per_z, quarter)], axis=1
    )
    returned = exchange(back, EP)

    slots = returned[:, :cap].reshape(n_ep * cap, quarter)
    position = expert_ids * cap + rank
    fetch = (position[:, :, None] == jnp.arange(n_ep * cap)).astype(BF)
    per_choice = dot32(fetch.reshape(rows * 2, n_ep * cap), slots).reshape(rows, 2, quarter)
    moe = jnp.sum(per_choice * route_weight[:, :, None], axis=1)
    branch = jnp.sum(
        returned[:, cap:].astype(F32).reshape(n_z, n_ep // n_z, per_z, quarter), axis=1
    ).reshape(rows, quarter)
    return (resid_own + moe + branch_weight[:, None] * branch).astype(BF)


def solution(mesh):
    torus = Mesh(mesh.devices.reshape(8, 8, 2, mesh.shape["tp"]), ("z", "y", "c", "x"))
    placed = (
        P(EP, None),
        P(EP, "x", None, None),
        P(),
        P(None, "x"),
        P(None, "x"),
        P(None, "x"),
        P(None, "x"),
        P(None, "x"),
        P("x"),
        P(),
        P("x", None),
        P(),
        P(EP, None),
        P(EP),
        P(EP, None),
        P(EP, None, "x"),
        P(EP, None, "x"),
        P(EP, "x", None),
        P(EP, "x"),
        P(EP, "x"),
        P(EP, "x"),
        P(),
    )
    return jax.shard_map(local, mesh=torus, in_specs=placed, out_specs=P(EP, "x"), check_vma=False)
```

```python
import jax
import jax.numpy as jnp
from jax import lax
from jax.experimental import pallas as pl
from jax.experimental.pallas import tpu as pltpu
from jax.sharding import Mesh
from jax.sharding import PartitionSpec as P

EP = ("z", "y", "c")
BF = jnp.bfloat16
F32 = jnp.float32


def rms_scale(values, gain, floor):
    return values * lax.rsqrt(jnp.mean(values * values, axis=-1, keepdims=True) + floor) * gain


def unit_rows(values):
    return values * lax.rsqrt(jnp.sum(values * values, axis=-1, keepdims=True) + 1.0)


def dot32(a, b):
    return jnp.dot(a, b, preferred_element_type=F32)


def mixer_body(
    hidden_ref,
    state_ref,
    gain_ref,
    query_ref,
    key_ref,
    value_ref,
    decay_ref,
    beta_ref,
    rate_ref,
    head_gain_ref,
    out_w_ref,
    partial_ref,
    read_q,
    read_k,
):
    rows, heads, dk, dv = state_ref.shape
    wide = hidden_ref[...].astype(F32)
    normed = rms_scale(wide, gain_ref[...], 0.1).astype(BF)
    wide = normed.astype(F32)
    q_all = dot32(normed, query_ref[...])
    k_all = dot32(normed, key_ref[...])
    units = []
    for source in (q_all, k_all):
        for h in range(heads):
            units.append(unit_rows(source[:, h * dk : (h + 1) * dk]))
    used = 2 * heads * rows
    stacked = jnp.concatenate(units + [jnp.zeros((dk - used, dk), F32)], axis=0)
    columns = stacked.T
    for h in range(heads):
        for s in range(rows):
            state = state_ref[s, h]
            q_col = columns[:, h * rows + s : h * rows + s + 1]
            k_at = (heads + h) * rows + s
            k_col = columns[:, k_at : k_at + 1]
            lanes = slice(h * dv, (h + 1) * dv)
            read_q[s : s + 1, lanes] = jnp.sum(state * q_col, axis=0, keepdims=True)
            read_k[s : s + 1, lanes] = jnp.sum(state * k_col, axis=0, keepdims=True)
    v_all = dot32(normed, value_ref[...])
    outs = []
    for h in range(heads):
        lanes = slice(h * dv, (h + 1) * dv)
        decay_in = jnp.sum(wide * decay_ref[h : h + 1, :].astype(F32), axis=1, keepdims=True)
        beta_in = jnp.sum(wide * beta_ref[h : h + 1, :].astype(F32), axis=1, keepdims=True)
        decay = jnp.exp(-rate_ref[h] * jax.nn.softplus(decay_in))
        meet = jnp.sum(units[h] * units[heads + h], axis=1, keepdims=True)
        meet = meet * jax.nn.sigmoid(beta_in)
        readout = decay * read_q[:, lanes] + meet * (v_all[:, lanes] - decay * read_k[:, lanes])
        outs.append(rms_scale(readout, head_gain_ref[...], 0.01).astype(BF))
    head_out = jnp.concatenate(outs, axis=1)
    partial_ref[...] = dot32(head_out, out_w_ref[...]).astype(BF)


def mixer(hidden, state, gain, query, key, value, decay, beta, rate, head_gain, out_w):
    rows, width = hidden.shape
    vmem = pl.BlockSpec(memory_space=pltpu.VMEM)
    smem = pl.BlockSpec(memory_space=pltpu.SMEM)
    wide = state.shape[1] * state.shape[3]
    return pl.pallas_call(
        mixer_body,
        out_shape=jax.ShapeDtypeStruct((rows, width), BF),
        in_specs=[vmem] * 8 + [smem] + [vmem] * 2,
        out_specs=vmem,
        scratch_shapes=[pltpu.VMEM((rows, wide), F32), pltpu.VMEM((rows, wide), F32)],
        name="mixer",
    )(
        hidden,
        state,
        gain[None],
        query,
        key,
        value,
        decay.T,
        beta.T,
        rate,
        head_gain[None],
        out_w,
    )


def exchange(blocks, axis):
    return lax.all_to_all(blocks, axis, split_axis=0, concat_axis=0, tiled=True)


def local(
    hidden_in,
    prior_state,
    mix_gain,
    query_w,
    key_w,
    value_w,
    decay_w,
    beta_w,
    decay_rate,
    head_gain,
    out_w,
    ffn_gain,
    expert_ids,
    group_share,
    expert_share,
    expert_gate,
    expert_up,
    expert_down,
    dense_gate,
    dense_up,
    dense_down,
    branch_gate,
):
    rows, width = hidden_in.shape
    n_ep = lax.axis_size(EP)
    n_tp = lax.axis_size("x")
    n_z = lax.axis_size("z")
    quarter = width // n_tp
    cap = 2
    per_z = rows // n_z
    tp_at = lax.axis_index("x")
    hid = dense_gate.shape[0]

    dense_all = jnp.concatenate([dense_gate, dense_up, dense_down], axis=0)
    copies = jnp.broadcast_to(dense_all, (n_z, *dense_all.shape))
    dense_z = exchange(copies, "z").reshape(n_z, 3, hid, quarter)

    partial_out = mixer(
        hidden_in,
        prior_state,
        mix_gain,
        query_w,
        key_w,
        value_w,
        decay_w,
        beta_w,
        decay_rate,
        head_gain,
        out_w,
    )
    partials = lax.all_gather(partial_out, "x")
    mix = jnp.sum(partials.astype(F32), axis=0)
    resid = (hidden_in.astype(F32) + mix).astype(BF)
    normed2 = rms_scale(resid.astype(F32), ffn_gain, 0.1).astype(BF)
    own = lax.dynamic_slice_in_dim(normed2, tp_at * quarter, quarter, 1)
    resid_own = lax.dynamic_slice_in_dim(resid, tp_at * quarter, quarter, 1).astype(F32)
    branch_weight = jax.nn.sigmoid(dot32(normed2, branch_gate))
    route_weight = (
        group_share[:, None] * expert_share / jnp.sum(expert_share, axis=1, keepdims=True)
    )

    same = expert_ids[:, :, None, None] == expert_ids[None, None, :, :]
    earlier = jnp.arange(rows)[:, None] > jnp.arange(rows)[None, :]
    rank = jnp.sum(same & earlier[:, None, :, None], axis=(2, 3)).astype(jnp.int32)
    dest = jnp.arange(n_ep)[:, None, None, None]
    slot = jnp.arange(cap)[None, :, None, None]
    chosen = (expert_ids[None, None] == dest) & (rank[None, None] == slot)
    pick_expert = jnp.any(chosen, axis=3)
    dense_row = (jnp.arange(n_ep) // (n_ep // n_z))[:, None] * per_z + jnp.arange(per_z)[None, :]
    pick_dense = dense_row[:, :, None] == jnp.arange(rows)
    pick = jnp.concatenate([pick_expert, pick_dense], axis=1).astype(BF)
    block = cap + per_z
    sent = dot32(pick.reshape(n_ep * block, rows), own).astype(BF)
    arrived = exchange(sent.reshape(n_ep, block, quarter), EP)
    moe_rows = arrived[:, :cap].reshape(n_ep * cap, quarter)
    dense_rows = arrived[:, cap:].reshape(n_ep * per_z, quarter)

    n_hid = n_z * hid
    gate_z = dense_z[:, 0].reshape(n_hid, quarter)
    up_z = dense_z[:, 1].reshape(n_hid, quarter)
    down_z = dense_z[:, 2].reshape(n_hid, quarter)
    contract = (((1,), (1,)), ((), ()))
    gate_part = lax.dot_general(dense_rows, gate_z, contract, preferred_element_type=F32)
    up_part = lax.dot_general(dense_rows, up_z, contract, preferred_element_type=F32)
    share = n_hid // n_tp
    pre = jnp.stack(
        [gate_part.reshape(-1, n_tp, share), up_part.reshape(-1, n_tp, share)], axis=2
    ).astype(BF)
    pre = jnp.moveaxis(pre, 1, 0).reshape(n_tp, -1, 2 * share)
    moe_copies = jnp.broadcast_to(moe_rows, (n_tp, *moe_rows.shape))
    first = exchange(jnp.concatenate([moe_copies, pre], axis=2), "x")

    full_rows = jnp.moveaxis(first[:, :, :quarter], 0, 1).reshape(n_ep * cap, width)
    pre_sum = jnp.sum(first[:, :, quarter:].astype(F32), axis=0)
    dense_hidden = (jax.nn.silu(pre_sum[:, :share]) * pre_sum[:, share:]).astype(BF)
    gate_pre = dot32(full_rows, expert_gate[0])
    up_pre = dot32(full_rows, expert_up[0])
    hidden = (jax.nn.silu(gate_pre) * up_pre).astype(BF)
    expert_part = dot32(hidden, expert_down[0]).astype(BF)
    part_blocks = jnp.moveaxis(expert_part.reshape(n_ep * cap, n_tp, quarter), 1, 0)
    hidden_copies = jnp.broadcast_to(dense_hidden, (n_tp, *dense_hidden.shape))
    second = exchange(jnp.concatenate([part_blocks, hidden_copies], axis=2), "x")

    expert_out = jnp.sum(second[:, :, :quarter].astype(F32), axis=0).astype(BF)
    all_hidden = jnp.moveaxis(second[:, :, quarter:], 0, 1).reshape(n_ep * per_z, n_hid)
    dense_out = dot32(all_hidden, down_z).astype(BF)
    back = jnp.concatenate(
        [expert_out.reshape(n_ep, cap, quarter), dense_out.reshape(n_ep, per_z, quarter)], axis=1
    )
    returned = exchange(back, EP)

    slots = returned[:, :cap].reshape(n_ep * cap, quarter)
    position = expert_ids * cap + rank
    fetch = (position[:, :, None] == jnp.arange(n_ep * cap)).astype(BF)
    per_choice = dot32(fetch.reshape(rows * 2, n_ep * cap), slots).reshape(rows, 2, quarter)
    moe = jnp.sum(per_choice * route_weight[:, :, None], axis=1)
    branch = jnp.sum(
        returned[:, cap:].astype(F32).reshape(n_z, n_ep // n_z, per_z, quarter), axis=1
    ).reshape(rows, quarter)
    return (resid_own + moe + branch_weight[:, None] * branch).astype(BF)


def solution(mesh):
    torus = Mesh(mesh.devices.reshape(8, 8, 2, mesh.shape["tp"]), ("z", "y", "c", "x"))
    placed = (
        P(EP, None),
        P(EP, "x", None, None),
        P(),
        P(None, "x"),
        P(None, "x"),
        P(None, "x"),
        P(None, "x"),
        P(None, "x"),
        P("x"),
        P(),
        P("x", None),
        P(),
        P(EP, None),
        P(EP),
        P(EP, None),
        P(EP, None, "x"),
        P(EP, None, "x"),
        P(EP, "x", None),
        P(EP, "x"),
        P(EP, "x"),
        P(EP, "x"),
        P(),
    )
    return jax.shard_map(local, mesh=torus, in_specs=placed, out_specs=P(EP, "x"), check_vma=False)
```

```python
import functools

import jax
import jax.numpy as jnp
from jax import lax
from jax.experimental import pallas as pl
from jax.experimental.pallas import tpu as pltpu
from jax.sharding import Mesh
from jax.sharding import PartitionSpec as P

EP = ("z", "y", "c")
BF = jnp.bfloat16
F32 = jnp.float32


def rms_scale(values, gain, floor):
    return values * lax.rsqrt(jnp.mean(values * values, axis=-1, keepdims=True) + floor) * gain


def unit_rows(values):
    return values * lax.rsqrt(jnp.sum(values * values, axis=-1, keepdims=True) + 1.0)


def dot32(a, b):
    return jnp.dot(a, b, preferred_element_type=F32)


def mixer_body(
    hidden_ref,
    gain_ref,
    decay_ref,
    beta_ref,
    rate_ref,
    head_gain_ref,
    query_hbm,
    key_hbm,
    value_hbm,
    out_w_hbm,
    state_hbm,
    partial_ref,
    query_ref,
    key_ref,
    value_ref,
    out_w_ref,
    state_ref,
    read_q,
    read_k,
    sems,
):
    rows, heads, dk, dv = state_ref.shape
    groups = 4
    step = rows // groups

    def fetch(source, target, at):
        return pltpu.make_async_copy(source, target, sems.at[at])

    get_query = fetch(query_hbm, query_ref, 0)
    get_key = fetch(key_hbm, key_ref, 1)
    get_value = fetch(value_hbm, value_ref, 2)
    get_out = fetch(out_w_hbm, out_w_ref, 3)
    get_state = [
        fetch(
            state_hbm.at[pl.ds(g * step, step)], state_ref.at[pl.ds(g * step, step)], 4 + g
        )
        for g in range(groups)
    ]
    for copy in [get_query, get_key] + get_state + [get_value, get_out]:
        copy.start()
    wide = hidden_ref[...].astype(F32)
    normed = rms_scale(wide, gain_ref[...], 0.1).astype(BF)
    wide = normed.astype(F32)
    get_query.wait()
    q_all = dot32(normed, query_ref[...])
    get_key.wait()
    k_all = dot32(normed, key_ref[...])
    units = []
    for source in (q_all, k_all):
        for h in range(heads):
            units.append(unit_rows(source[:, h * dk : (h + 1) * dk]))
    used = 2 * heads * rows
    stacked = jnp.concatenate(units + [jnp.zeros((dk - used, dk), F32)], axis=0)
    columns = stacked.T
    for g in range(groups):
        get_state[g].wait()
        for s in range(g * step, (g + 1) * step):
            for h in range(heads):
                state = state_ref[s, h]
                q_col = columns[:, h * rows + s : h * rows + s + 1]
                k_at = (heads + h) * rows + s
                k_col = columns[:, k_at : k_at + 1]
                lanes = slice(h * dv, (h + 1) * dv)
                read_q[s : s + 1, lanes] = jnp.sum(state * q_col, axis=0, keepdims=True)
                read_k[s : s + 1, lanes] = jnp.sum(state * k_col, axis=0, keepdims=True)
    get_value.wait()
    v_all = dot32(normed, value_ref[...])
    outs = []
    for h in range(heads):
        lanes = slice(h * dv, (h + 1) * dv)
        decay_in = jnp.sum(wide * decay_ref[h : h + 1, :].astype(F32), axis=1, keepdims=True)
        beta_in = jnp.sum(wide * beta_ref[h : h + 1, :].astype(F32), axis=1, keepdims=True)
        decay = jnp.exp(-rate_ref[h] * jax.nn.softplus(decay_in))
        meet = jnp.sum(units[h] * units[heads + h], axis=1, keepdims=True)
        meet = meet * jax.nn.sigmoid(beta_in)
        readout = decay * read_q[:, lanes] + meet * (v_all[:, lanes] - decay * read_k[:, lanes])
        outs.append(rms_scale(readout, head_gain_ref[...], 0.01).astype(BF))
    head_out = jnp.concatenate(outs, axis=1)
    get_out.wait()
    partial_ref[...] = dot32(head_out, out_w_ref[...]).astype(BF)


def mixer(hidden, state, gain, query, key, value, decay, beta, rate, head_gain, out_w):
    rows, width = hidden.shape
    vmem = pl.BlockSpec(memory_space=pltpu.VMEM)
    smem = pl.BlockSpec(memory_space=pltpu.SMEM)
    hbm = pl.BlockSpec(memory_space=pl.ANY)
    wide = state.shape[1] * state.shape[3]
    return pl.pallas_call(
        mixer_body,
        out_shape=jax.ShapeDtypeStruct((rows, width), BF),
        in_specs=[vmem] * 4 + [smem, vmem] + [hbm] * 5,
        out_specs=vmem,
        scratch_shapes=[
            pltpu.VMEM(query.shape, BF),
            pltpu.VMEM(key.shape, BF),
            pltpu.VMEM(value.shape, BF),
            pltpu.VMEM(out_w.shape, BF),
            pltpu.VMEM(state.shape, F32),
            pltpu.VMEM((rows, wide), F32),
            pltpu.VMEM((rows, wide), F32),
            pltpu.SemaphoreType.DMA((8,)),
        ],
        name="mixer",
    )(
        hidden,
        gain[None],
        decay.T,
        beta.T,
        rate,
        head_gain[None],
        query,
        key,
        value,
        out_w,
        state,
    )


def spread_body(*refs):
    sources, target, sems = refs[:-2], refs[-2], refs[-1]
    rows = sources[0].shape[0]
    started = []
    for c in range(target.shape[0]):
        for w, source in enumerate(sources):
            copy = pltpu.make_async_copy(
                source, target.at[c, pl.ds(w * rows, rows)], sems.at[c * len(sources) + w]
            )
            copy.start()
            started.append(copy)
    for copy in started:
        copy.wait()


def spread(weights, count):
    rows, width = weights[0].shape
    hbm = pl.BlockSpec(memory_space=pl.ANY)
    return pl.pallas_call(
        spread_body,
        out_shape=jax.ShapeDtypeStruct((count, len(weights) * rows, width), BF),
        in_specs=[hbm] * len(weights),
        out_specs=hbm,
        scratch_shapes=[pltpu.SemaphoreType.DMA((count * len(weights),))],
        name="spread",
    )(*weights)


def prepare_body(
    n_ep,
    n_z,
    tp_ref,
    partials_ref,
    hidden_ref,
    gain_ref,
    branch_ref,
    ids_ref,
    sent_ref,
    resid_ref,
    weight_ref,
    position_ref,
):
    rows, width = hidden_ref.shape
    quarter = resid_ref.shape[1]
    n_tp = width // quarter
    choices = ids_ref.shape[0]
    half = quarter // 2
    mix = partials_ref[:rows].astype(F32)
    for t in range(1, n_tp):
        mix = mix + partials_ref[t * rows : (t + 1) * rows].astype(F32)
    resid = (hidden_ref[...].astype(F32) + mix).astype(BF).astype(F32)
    normed = rms_scale(resid, gain_ref[...], 0.1).astype(BF)
    wide = normed.astype(F32)
    dot = jnp.sum(wide * branch_ref[...].astype(F32), axis=1, keepdims=True)
    weight_ref[...] = jnp.broadcast_to(jax.nn.sigmoid(dot), weight_ref.shape)
    tp_at = tp_ref[0]
    own = wide[:, :quarter]
    resid_own = resid[:, :quarter]
    for t in range(1, n_tp):
        here = tp_at == t
        own = jnp.where(here, wide[:, t * quarter : (t + 1) * quarter], own)
        resid_own = jnp.where(here, resid[:, t * quarter : (t + 1) * quarter], resid_own)
    resid_ref[...] = resid_own

    row_ids = ids_ref[...].astype(F32)
    r_at = lax.broadcasted_iota(jnp.int32, (rows, rows), 0)
    c_at = lax.broadcasted_iota(jnp.int32, (rows, rows), 1)
    eye = jnp.where(r_at == c_at, 1.0, 0.0)
    col_ids = lax.dot_general(
        eye, row_ids, (((1,), (1,)), ((), ())), preferred_element_type=F32
    )
    row_pos, col_pos = [], []
    for j in range(choices):
        by_row = jnp.zeros((rows, rows), F32)
        by_col = jnp.zeros((rows, rows), F32)
        for o in range(choices):
            by_row += jnp.where(col_ids[:, o : o + 1] == row_ids[j : j + 1, :], 1.0, 0.0)
            by_col += jnp.where(col_ids[:, j : j + 1] == row_ids[o : o + 1, :], 1.0, 0.0)
        row_rank = jnp.sum(jnp.where(r_at < c_at, by_row, 0.0), axis=0, keepdims=True)
        col_rank = jnp.sum(jnp.where(c_at < r_at, by_col, 0.0), axis=1, keepdims=True)
        row_pos.append(row_ids[j : j + 1, :] * 2.0 + row_rank)
        col_pos.append(col_ids[:, j : j + 1] * 2.0 + col_rank)
    lane = lax.broadcasted_iota(jnp.int32, position_ref.shape, 1)
    position_ref[...] = jnp.where(lane == 0, col_pos[0], col_pos[1]).astype(jnp.int32)

    shape = (n_ep * 8, 2 * rows)
    at = lax.broadcasted_iota(jnp.int32, shape, 0)
    col = lax.broadcasted_iota(jnp.int32, shape, 1)
    slot = at & 1
    dest = at >> 3
    expert_key = (dest * 2 + slot).astype(F32)
    dense_key = (dest // (n_ep // n_z)) * 2 + slot
    for_expert = (at & 2) == 0
    same_half = ((at >> 2) & 1) == jnp.where(col >= rows, 1, 0)
    token = jnp.where(col >= rows, col - rows, col)
    first = jnp.concatenate([row_pos[0], row_pos[0]], axis=1)
    second = jnp.concatenate([row_pos[1], row_pos[1]], axis=1)
    expert_hit = jnp.where(
        (expert_key == first) | (expert_key == second), 1.0, 0.0
    )
    dense_hit = jnp.where(dense_key == token, 1.0, 0.0)
    pick = jnp.where(same_half, jnp.where(for_expert, expert_hit, dense_hit), 0.0).astype(BF)
    halves = jnp.concatenate([own[:, :half], own[:, half:]], axis=0).astype(BF)
    sent_ref[...] = dot32(pick, halves).astype(BF)


def prepare(tp_at, partials, hidden, gain, branch_gate, ids, n_ep, n_z, n_tp):
    rows, width = hidden.shape
    quarter = width // n_tp
    vmem = pl.BlockSpec(memory_space=pltpu.VMEM)
    return pl.pallas_call(
        functools.partial(prepare_body, n_ep, n_z),
        out_shape=(
            jax.ShapeDtypeStruct((n_ep * 8, quarter // 2), BF),
            jax.ShapeDtypeStruct((rows, quarter), F32),
            jax.ShapeDtypeStruct((rows, 128), F32),
            jax.ShapeDtypeStruct((rows, 128), jnp.int32),
        ),
        in_specs=[pl.BlockSpec(memory_space=pltpu.SMEM)] + [vmem] * 5,
        out_specs=(vmem,) * 4,
        name="prepare",
    )(tp_at, partials, hidden, gain[None], branch_gate[None], ids.T)


def exchange(blocks, axis):
    return lax.all_to_all(blocks, axis, split_axis=0, concat_axis=0, tiled=True)


def local(
    hidden_in,
    prior_state,
    mix_gain,
    query_w,
    key_w,
    value_w,
    decay_w,
    beta_w,
    decay_rate,
    head_gain,
    out_w,
    ffn_gain,
    expert_ids,
    group_share,
    expert_share,
    expert_gate,
    expert_up,
    expert_down,
    dense_gate,
    dense_up,
    dense_down,
    branch_gate,
):
    rows, width = hidden_in.shape
    n_ep = lax.axis_size(EP)
    n_tp = lax.axis_size("x")
    n_z = lax.axis_size("z")
    quarter = width // n_tp
    cap = 2
    per_z = rows // n_z
    tp_at = lax.axis_index("x")
    hid = dense_gate.shape[0]

    copies = spread((dense_gate, dense_up, dense_down), n_z)
    dense_z = exchange(copies, "z").reshape(n_z, 3, hid, quarter)

    partial_out = mixer(
        hidden_in,
        prior_state,
        mix_gain,
        query_w,
        key_w,
        value_w,
        decay_w,
        beta_w,
        decay_rate,
        head_gain,
        out_w,
    )
    partials = lax.all_gather(partial_out, "x", axis=0, tiled=True)
    sent, resid_own, branch_weight, position = prepare(
        tp_at[None], partials, hidden_in, ffn_gain, branch_gate, expert_ids, n_ep, n_z, n_tp
    )
    branch_weight = branch_weight[:, :1]
    position = position[:, :2]
    block = cap + per_z
    arrived = exchange(sent.reshape(n_ep, 8, quarter // 2), EP)
    arrived = arrived.reshape(n_ep, 2, block, quarter // 2)
    arrived = jnp.concatenate([arrived[:, 0], arrived[:, 1]], axis=2)
    moe_rows = arrived[:, :cap].reshape(n_ep * cap, quarter)
    dense_rows = arrived[:, cap:].reshape(n_ep * per_z, quarter)

    n_hid = n_z * hid
    gate_z = dense_z[:, 0].reshape(n_hid, quarter)
    up_z = dense_z[:, 1].reshape(n_hid, quarter)
    down_z = dense_z[:, 2].reshape(n_hid, quarter)
    contract = (((1,), (1,)), ((), ()))
    gate_part = lax.dot_general(dense_rows, gate_z, contract, preferred_element_type=F32)
    up_part = lax.dot_general(dense_rows, up_z, contract, preferred_element_type=F32)
    share = n_hid // n_tp
    pre = jnp.stack(
        [gate_part.reshape(-1, n_tp, share), up_part.reshape(-1, n_tp, share)], axis=2
    ).astype(BF)
    pre = jnp.moveaxis(pre, 1, 0).reshape(n_tp, -1, 2 * share)
    moe_copies = jnp.broadcast_to(moe_rows, (n_tp, *moe_rows.shape))
    first = exchange(jnp.concatenate([moe_copies, pre], axis=2), "x")

    full_rows = jnp.moveaxis(first[:, :, :quarter], 0, 1).reshape(n_ep * cap, width)
    pre_sum = jnp.sum(first[:, :, quarter:].astype(F32), axis=0)
    dense_hidden = (jax.nn.silu(pre_sum[:, :share]) * pre_sum[:, share:]).astype(BF)
    gate_pre = dot32(full_rows, expert_gate[0])
    up_pre = dot32(full_rows, expert_up[0])
    hidden = (jax.nn.silu(gate_pre) * up_pre).astype(BF)
    expert_part = dot32(hidden, expert_down[0]).astype(BF)
    part_blocks = jnp.moveaxis(expert_part.reshape(n_ep * cap, n_tp, quarter), 1, 0)
    hidden_copies = jnp.broadcast_to(dense_hidden, (n_tp, *dense_hidden.shape))
    second = exchange(jnp.concatenate([part_blocks, hidden_copies], axis=2), "x")

    expert_out = jnp.sum(second[:, :, :quarter].astype(F32), axis=0).astype(BF)
    all_hidden = jnp.moveaxis(second[:, :, quarter:], 0, 1).reshape(n_ep * per_z, n_hid)
    dense_out = dot32(all_hidden, down_z).astype(BF)
    back = jnp.concatenate(
        [expert_out.reshape(n_ep, cap, quarter), dense_out.reshape(n_ep, per_z, quarter)], axis=1
    )
    returned = exchange(back, EP)

    slots = returned[:, :cap].reshape(n_ep * cap, quarter)
    route_weight = (
        group_share[:, None] * expert_share / jnp.sum(expert_share, axis=1, keepdims=True)
    )
    fetch = (position[:, :, None] == jnp.arange(n_ep * cap)).astype(BF)
    per_choice = dot32(fetch.reshape(rows * 2, n_ep * cap), slots).reshape(rows, 2, quarter)
    moe = jnp.sum(per_choice * route_weight[:, :, None], axis=1)
    branch = jnp.sum(
        returned[:, cap:].astype(F32).reshape(n_z, n_ep // n_z, per_z, quarter), axis=1
    ).reshape(rows, quarter)
    return (resid_own + moe + branch_weight * branch).astype(BF)


def solution(mesh):
    torus = Mesh(mesh.devices.reshape(8, 8, 2, mesh.shape["tp"]), ("z", "y", "c", "x"))
    placed = (
        P(EP, None),
        P(EP, "x", None, None),
        P(),
        P(None, "x"),
        P(None, "x"),
        P(None, "x"),
        P(None, "x"),
        P(None, "x"),
        P("x"),
        P(),
        P("x", None),
        P(),
        P(EP, None),
        P(EP),
        P(EP, None),
        P(EP, None, "x"),
        P(EP, None, "x"),
        P(EP, "x", None),
        P(EP, "x"),
        P(EP, "x"),
        P(EP, "x"),
        P(),
    )
    return jax.shard_map(local, mesh=torus, in_specs=placed, out_specs=P(EP, "x"), check_vma=False)
```

```python
import jax
import jax.numpy as jnp
from jax import lax
from jax.experimental import pallas as pl
from jax.experimental.pallas import tpu as pltpu
from jax.sharding import Mesh
from jax.sharding import PartitionSpec as P

EP = ("z", "y", "c")
BF = jnp.bfloat16
F32 = jnp.float32


def rms_scale(values, gain, floor):
    return values * lax.rsqrt(jnp.mean(values * values, axis=-1, keepdims=True) + floor) * gain


def unit_rows(values):
    return values * lax.rsqrt(jnp.sum(values * values, axis=-1, keepdims=True) + 1.0)


def dot32(a, b):
    return jnp.dot(a, b, preferred_element_type=F32)


def slots_of(ids_ref, row_slot_ref, col_slot_ref, rows):
    choices = ids_ref.shape[0]
    row_ids = ids_ref[...].astype(F32)
    r_at = lax.broadcasted_iota(jnp.int32, (rows, rows), 0)
    c_at = lax.broadcasted_iota(jnp.int32, (rows, rows), 1)
    eye = jnp.where(r_at == c_at, 1.0, 0.0)
    col_ids = lax.dot_general(eye, row_ids, (((1,), (1,)), ((), ())), preferred_element_type=F32)
    row_slots, col_slots = [], []
    for j in range(choices):
        by_row = jnp.zeros((rows, rows), F32)
        by_col = jnp.zeros((rows, rows), F32)
        for o in range(choices):
            by_row += jnp.where(col_ids[:, o : o + 1] == row_ids[j : j + 1, :], 1.0, 0.0)
            by_col += jnp.where(col_ids[:, j : j + 1] == row_ids[o : o + 1, :], 1.0, 0.0)
        row_rank = jnp.sum(jnp.where(r_at < c_at, by_row, 0.0), axis=0, keepdims=True)
        col_rank = jnp.sum(jnp.where(c_at < r_at, by_col, 0.0), axis=1, keepdims=True)
        row_slots.append(row_ids[j : j + 1, :] * 2.0 + row_rank)
        col_slots.append(col_ids[:, j : j + 1] * 2.0 + col_rank)
    row_slot_ref[...] = jnp.concatenate(row_slots, axis=0).astype(jnp.int32)
    col_slot_ref[...] = jnp.concatenate(col_slots, axis=1).astype(jnp.int32)


def mixer_body(
    hidden_ref,
    gain_ref,
    decay_ref,
    beta_ref,
    rate_ref,
    head_gain_ref,
    ids_ref,
    query_hbm,
    key_hbm,
    value_hbm,
    out_w_hbm,
    state_hbm,
    partial_ref,
    row_slot_ref,
    col_slot_ref,
    query_ref,
    key_ref,
    value_ref,
    out_w_ref,
    state_ref,
    sems,
):
    rows = hidden_ref.shape[0]
    heads = decay_ref.shape[0]
    dv = head_gain_ref.shape[1]
    dk = query_ref.shape[1] // heads
    groups = 4
    step = state_ref.shape[0] // groups

    def fetch(source, target, at):
        return pltpu.make_async_copy(source, target, sems.at[at])

    get_query = fetch(query_hbm, query_ref, 0)
    get_key = fetch(key_hbm, key_ref, 1)
    get_value = fetch(value_hbm, value_ref, 2)
    get_out = fetch(out_w_hbm, out_w_ref, 3)
    get_state = [
        fetch(
            state_hbm.at[pl.ds(g * step, step)], state_ref.at[pl.ds(g * step, step)], 4 + g
        )
        for g in range(groups)
    ]
    for copy in [get_query, get_key] + get_state + [get_value, get_out]:
        copy.start()
    slots_of(ids_ref, row_slot_ref, col_slot_ref, rows)
    wide = hidden_ref[...].astype(F32)
    normed = rms_scale(wide, gain_ref[...], 0.1).astype(BF)
    wide = normed.astype(F32)
    get_query.wait()
    q_all = dot32(normed, query_ref[...])
    get_key.wait()
    k_all = dot32(normed, key_ref[...])
    units = []
    for source in (q_all, k_all):
        for h in range(heads):
            units.append(unit_rows(source[:, h * dk : (h + 1) * dk]))
    stacked = jnp.concatenate(units, axis=0).astype(BF)
    pairs = heads * rows
    row_at = lax.broadcasted_iota(jnp.int32, stacked.shape, 0) % pairs
    zero = jnp.zeros_like(stacked)
    read = jnp.zeros((2 * pairs, dv), F32)
    for g in range(groups):
        get_state[g].wait()
        blocks = []
        for b in range(g * step // dk, (g + 1) * step // dk):
            blocks.append(jnp.where(row_at == (b % heads) * rows + b // heads, stacked, zero))
        state = state_ref[g * step : (g + 1) * step].astype(BF)
        read = read + dot32(jnp.concatenate(blocks, axis=1), state)
    get_value.wait()
    v_all = dot32(normed, value_ref[...])
    outs = []
    for h in range(heads):
        lanes = slice(h * dv, (h + 1) * dv)
        decay_in = jnp.sum(wide * decay_ref[h : h + 1, :].astype(F32), axis=1, keepdims=True)
        beta_in = jnp.sum(wide * beta_ref[h : h + 1, :].astype(F32), axis=1, keepdims=True)
        decay = jnp.exp(-rate_ref[h] * jax.nn.softplus(decay_in))
        meet = jnp.sum(units[h] * units[heads + h], axis=1, keepdims=True)
        meet = meet * jax.nn.sigmoid(beta_in)
        read_q = read[h * rows : (h + 1) * rows]
        read_k = read[pairs + h * rows : pairs + (h + 1) * rows]
        readout = decay * read_q + meet * (v_all[:, lanes] - decay * read_k)
        outs.append(rms_scale(readout, head_gain_ref[...], 0.01).astype(BF))
    head_out = jnp.concatenate(outs, axis=1)
    get_out.wait()
    partial_ref[...] = dot32(head_out, out_w_ref[...]).astype(BF)


def mixer(hidden, state, gain, query, key, value, decay, beta, rate, head_gain, out_w, ids):
    rows, width = hidden.shape
    vmem = pl.BlockSpec(memory_space=pltpu.VMEM)
    smem = pl.BlockSpec(memory_space=pltpu.SMEM)
    hbm = pl.BlockSpec(memory_space=pl.ANY)
    state = state.reshape(-1, state.shape[-1])
    return pl.pallas_call(
        mixer_body,
        out_shape=(
            jax.ShapeDtypeStruct((rows, width), BF),
            jax.ShapeDtypeStruct(ids.shape[::-1], jnp.int32),
            jax.ShapeDtypeStruct(ids.shape, jnp.int32),
        ),
        in_specs=[vmem] * 4 + [smem, vmem, vmem] + [hbm] * 5,
        out_specs=(vmem,) * 3,
        scratch_shapes=[
            pltpu.VMEM(query.shape, BF),
            pltpu.VMEM(key.shape, BF),
            pltpu.VMEM(value.shape, BF),
            pltpu.VMEM(out_w.shape, BF),
            pltpu.VMEM(state.shape, F32),
            pltpu.SemaphoreType.DMA((8,)),
        ],
        name="mixer",
    )(
        hidden,
        gain[None],
        decay.T,
        beta.T,
        rate,
        head_gain[None],
        ids.T,
        query,
        key,
        value,
        out_w,
        state,
    )


def spread_body(*refs):
    sources, target = refs[:-1], refs[-1]
    rows = sources[0].shape[0]
    for w, source in enumerate(sources):
        for c in range(target.shape[0]):
            target[c, w * rows : (w + 1) * rows, :] = source[...]


def spread(weights, count):
    rows, width = weights[0].shape
    vmem = pl.BlockSpec(memory_space=pltpu.VMEM)
    return pl.pallas_call(
        spread_body,
        out_shape=jax.ShapeDtypeStruct((count, len(weights) * rows, width), BF),
        in_specs=[vmem] * len(weights),
        out_specs=vmem,
        name="spread",
    )(*weights)


def exchange(blocks, axis):
    return lax.all_to_all(blocks, axis, split_axis=0, concat_axis=0, tiled=True)


def local(
    hidden_in,
    prior_state,
    mix_gain,
    query_w,
    key_w,
    value_w,
    decay_w,
    beta_w,
    decay_rate,
    head_gain,
    out_w,
    ffn_gain,
    expert_ids,
    group_share,
    expert_share,
    expert_gate,
    expert_up,
    expert_down,
    dense_gate,
    dense_up,
    dense_down,
    branch_gate,
):
    rows, width = hidden_in.shape
    n_ep = lax.axis_size(EP)
    n_tp = lax.axis_size("x")
    n_z = lax.axis_size("z")
    quarter = width // n_tp
    cap = 2
    per_z = rows // n_z
    tp_at = lax.axis_index("x")
    hid = dense_gate.shape[0]

    copies = spread((dense_gate, dense_up, dense_down), n_z)
    dense_z = exchange(copies, "z").reshape(n_z, 3, hid, quarter)

    partial_out, row_slot, position = mixer(
        hidden_in,
        prior_state,
        mix_gain,
        query_w,
        key_w,
        value_w,
        decay_w,
        beta_w,
        decay_rate,
        head_gain,
        out_w,
        expert_ids,
    )
    partials = lax.all_gather(partial_out, "x", axis=0, tiled=True)
    partials = partials.reshape(n_tp, rows, width)
    mix = jnp.sum(partials.astype(F32), axis=0)
    resid = (hidden_in.astype(F32) + mix).astype(BF)
    normed2 = rms_scale(resid.astype(F32), ffn_gain, 0.1).astype(BF)
    own = lax.dynamic_slice_in_dim(normed2, tp_at * quarter, quarter, 1)
    resid_own = lax.dynamic_slice_in_dim(resid, tp_at * quarter, quarter, 1).astype(F32)
    branch_weight = jax.nn.sigmoid(dot32(normed2, branch_gate))[:, None]

    block = cap + per_z
    at = jnp.arange(n_ep * 2 * block)[:, None]
    dest, slot = at // (2 * block), at % cap
    col = jnp.arange(2 * rows)[None, :]
    slots = jnp.concatenate([row_slot, row_slot], axis=1)
    expert_at = dest * cap + slot
    expert_hit = (slots[:1] == expert_at) | (slots[1:] == expert_at)
    dense_hit = col % rows == dest // (n_ep // n_z) * per_z + slot
    hit = jnp.where(at % block < cap, expert_hit, dense_hit)
    pick = (hit & (at % (2 * block) // block == col // rows)).astype(BF)
    halves = jnp.concatenate([own[:, : quarter // 2], own[:, quarter // 2 :]], axis=0)
    sent = dot32(pick, halves).astype(BF)
    arrived = exchange(sent.reshape(n_ep, 8, quarter // 2), EP)
    arrived = arrived.reshape(n_ep, 2, block, quarter // 2)
    arrived = jnp.concatenate([arrived[:, 0], arrived[:, 1]], axis=2)
    moe_rows = arrived[:, :cap].reshape(n_ep * cap, quarter)
    dense_rows = arrived[:, cap:].reshape(n_ep * per_z, quarter)

    n_hid = n_z * hid
    gate_z = dense_z[:, 0].reshape(n_hid, quarter)
    up_z = dense_z[:, 1].reshape(n_hid, quarter)
    down_z = dense_z[:, 2].reshape(n_hid, quarter)
    contract = (((1,), (1,)), ((), ()))
    gate_part = lax.dot_general(dense_rows, gate_z, contract, preferred_element_type=F32)
    up_part = lax.dot_general(dense_rows, up_z, contract, preferred_element_type=F32)
    share = n_hid // n_tp
    pre = jnp.stack(
        [gate_part.reshape(-1, n_tp, share), up_part.reshape(-1, n_tp, share)], axis=2
    ).astype(BF)
    pre = jnp.moveaxis(pre, 1, 0).reshape(n_tp, -1, 2 * share)
    moe_copies = jnp.broadcast_to(moe_rows, (n_tp, *moe_rows.shape))
    first = exchange(jnp.concatenate([moe_copies, pre], axis=2), "x")

    full_rows = jnp.moveaxis(first[:, :, :quarter], 0, 1).reshape(n_ep * cap, width)
    pre_sum = jnp.sum(first[:, :, quarter:].astype(F32), axis=0)
    dense_hidden = (jax.nn.silu(pre_sum[:, :share]) * pre_sum[:, share:]).astype(BF)
    gate_pre = dot32(full_rows, expert_gate[0])
    up_pre = dot32(full_rows, expert_up[0])
    hidden = (jax.nn.silu(gate_pre) * up_pre).astype(BF)
    expert_part = dot32(hidden, expert_down[0]).astype(BF)
    part_blocks = jnp.moveaxis(expert_part.reshape(n_ep * cap, n_tp, quarter), 1, 0)
    hidden_copies = jnp.broadcast_to(dense_hidden, (n_tp, *dense_hidden.shape))
    second = exchange(jnp.concatenate([part_blocks, hidden_copies], axis=2), "x")

    expert_out = jnp.sum(second[:, :, :quarter].astype(F32), axis=0).astype(BF)
    all_hidden = jnp.moveaxis(second[:, :, quarter:], 0, 1).reshape(n_ep * per_z, n_hid)
    dense_out = dot32(all_hidden, down_z).astype(BF)
    back = jnp.concatenate(
        [expert_out.reshape(n_ep, cap, quarter), dense_out.reshape(n_ep, per_z, quarter)], axis=1
    )
    returned = exchange(back, EP)

    slots = returned[:, :cap].reshape(n_ep * cap, quarter)
    route_weight = (
        group_share[:, None] * expert_share / jnp.sum(expert_share, axis=1, keepdims=True)
    )
    fetch = (position[:, :, None] == jnp.arange(n_ep * cap)).astype(BF)
    per_choice = dot32(fetch.reshape(rows * 2, n_ep * cap), slots).reshape(rows, 2, quarter)
    moe = jnp.sum(per_choice * route_weight[:, :, None], axis=1)
    branch = jnp.sum(
        returned[:, cap:].astype(F32).reshape(n_z, n_ep // n_z, per_z, quarter), axis=1
    ).reshape(rows, quarter)
    return (resid_own + moe + branch_weight * branch).astype(BF)


def solution(mesh):
    torus = Mesh(mesh.devices.reshape(8, 8, 2, mesh.shape["tp"]), ("z", "y", "c", "x"))
    placed = (
        P(EP, None),
        P(EP, "x", None, None),
        P(),
        P(None, "x"),
        P(None, "x"),
        P(None, "x"),
        P(None, "x"),
        P(None, "x"),
        P("x"),
        P(),
        P("x", None),
        P(),
        P(EP, None),
        P(EP),
        P(EP, None),
        P(EP, None, "x"),
        P(EP, None, "x"),
        P(EP, "x", None),
        P(EP, "x"),
        P(EP, "x"),
        P(EP, "x"),
        P(),
    )
    return jax.shard_map(local, mesh=torus, in_specs=placed, out_specs=P(EP, "x"), check_vma=False)
```

```python
import functools

import jax
import jax.numpy as jnp
from jax import lax
from jax.experimental import pallas as pl
from jax.experimental.pallas import tpu as pltpu
from jax.sharding import Mesh
from jax.sharding import PartitionSpec as P

EP = ("z_hi", "z_lo", "y_hi", "y_lo", "c")
NEAR = ("z_lo", "y_lo", "c")
BF = jnp.bfloat16
F32 = jnp.float32


def rms_scale(values, gain, floor):
    return values * lax.rsqrt(jnp.mean(values * values, axis=-1, keepdims=True) + floor) * gain


def unit_rows(values):
    return values * lax.rsqrt(jnp.sum(values * values, axis=-1, keepdims=True) + 1.0)


def dot32(a, b):
    return jnp.dot(a, b, preferred_element_type=F32)


def slots_of(ids_ref, pick_ref, slot_ref, near, rows):
    choices = ids_ref.shape[0]
    row_ids = ids_ref[...].astype(F32)
    r_at = lax.broadcasted_iota(jnp.int32, (rows, rows), 0)
    c_at = lax.broadcasted_iota(jnp.int32, (rows, rows), 1)
    eye = jnp.where(r_at == c_at, 1.0, 0.0)
    col_ids = lax.dot_general(eye, row_ids, (((1,), (1,)), ((), ())), preferred_element_type=F32)
    row_slots, col_slots = [], []
    for j in range(choices):
        by_row = jnp.zeros((rows, rows), F32)
        by_col = jnp.zeros((rows, rows), F32)
        for o in range(choices):
            by_row += jnp.where(col_ids[:, o : o + 1] == row_ids[j : j + 1, :], 1.0, 0.0)
            by_col += jnp.where(col_ids[:, j : j + 1] == row_ids[o : o + 1, :], 1.0, 0.0)
        row_rank = jnp.sum(jnp.where(r_at < c_at, by_row, 0.0), axis=0, keepdims=True)
        col_rank = jnp.sum(jnp.where(c_at < r_at, by_col, 0.0), axis=1, keepdims=True)
        row_slots.append(row_ids[j : j + 1, :] * 2.0 + row_rank)
        col_slots.append(col_ids[:, j : j + 1] * 2.0 + col_rank)
    slot_ref[...] = jnp.concatenate(col_slots, axis=1).astype(jnp.int32)

    shape = (8, 2 * rows)
    at = lax.broadcasted_iota(jnp.int32, shape, 0)
    col = lax.broadcasted_iota(jnp.int32, shape, 1)
    slot = (at & 1).astype(F32)
    same_half = (at >= 4) == (col >= rows)
    for_expert = (at & 2) == 0
    token = jnp.where(col >= rows, col - rows, col).astype(F32)
    expert_keys = [
        jnp.where(
            same_half & for_expert, jnp.concatenate([found, found], axis=1) - slot, -1.0
        )
        for found in row_slots
    ]
    dense_key = jnp.where(same_half, jnp.where(for_expert, -1.0, token - slot), -1.0)
    dense_hit = [dense_key == 2.0 * n for n in range(near)]
    blocks = []
    for d in range(pick_ref.shape[0] // 8):
        hit = dense_hit[d // 16 % 2 * 4 + d // 2 % 2 * 2 + d % 2]
        for key in expert_keys:
            hit = hit | (key == 2.0 * d)
        blocks.append(jnp.where(hit, 1.0, 0.0))
    pick_ref[...] = jnp.concatenate(blocks, axis=0).astype(BF)


def mixer_body(
    near,
    hidden_ref,
    gain_ref,
    decay_ref,
    beta_ref,
    rate_ref,
    head_gain_ref,
    ids_ref,
    query_hbm,
    key_hbm,
    value_hbm,
    out_w_hbm,
    state_hbm,
    partial_ref,
    pick_ref,
    slot_ref,
    query_ref,
    key_ref,
    value_ref,
    out_w_ref,
    state_ref,
    sems,
):
    rows = hidden_ref.shape[0]
    heads = decay_ref.shape[0]
    dv = head_gain_ref.shape[1]
    dk = query_ref.shape[1] // heads
    groups = 4
    step = state_ref.shape[0] // groups

    def fetch(source, target, at):
        return pltpu.make_async_copy(source, target, sems.at[at])

    get_query = fetch(query_hbm, query_ref, 0)
    get_key = fetch(key_hbm, key_ref, 1)
    get_value = fetch(value_hbm, value_ref, 2)
    get_out = fetch(out_w_hbm, out_w_ref, 3)
    get_state = [
        fetch(
            state_hbm.at[pl.ds(g * step, step)], state_ref.at[pl.ds(g * step, step)], 4 + g
        )
        for g in range(groups)
    ]
    for copy in [get_query, get_key] + get_state + [get_value, get_out]:
        copy.start()
    slots_of(ids_ref, pick_ref, slot_ref, near, rows)
    wide = hidden_ref[...].astype(F32)
    normed = rms_scale(wide, gain_ref[...], 0.1).astype(BF)
    wide = normed.astype(F32)
    get_query.wait()
    q_all = dot32(normed, query_ref[...])
    get_key.wait()
    k_all = dot32(normed, key_ref[...])
    units = []
    for source in (q_all, k_all):
        for h in range(heads):
            units.append(unit_rows(source[:, h * dk : (h + 1) * dk]))
    stacked = jnp.concatenate(units, axis=0).astype(BF)
    pairs = heads * rows
    row_at = lax.broadcasted_iota(jnp.int32, stacked.shape, 0) % pairs
    zero = jnp.zeros_like(stacked)
    read = jnp.zeros((2 * pairs, dv), F32)
    for g in range(groups):
        get_state[g].wait()
        blocks = []
        for b in range(g * step // dk, (g + 1) * step // dk):
            blocks.append(jnp.where(row_at == (b % heads) * rows + b // heads, stacked, zero))
        state = state_ref[g * step : (g + 1) * step].astype(BF)
        read = read + dot32(jnp.concatenate(blocks, axis=1), state)
    get_value.wait()
    v_all = dot32(normed, value_ref[...])
    outs = []
    for h in range(heads):
        lanes = slice(h * dv, (h + 1) * dv)
        decay_in = jnp.sum(wide * decay_ref[h : h + 1, :].astype(F32), axis=1, keepdims=True)
        beta_in = jnp.sum(wide * beta_ref[h : h + 1, :].astype(F32), axis=1, keepdims=True)
        decay = jnp.exp(-rate_ref[h] * jax.nn.softplus(decay_in))
        meet = jnp.sum(units[h] * units[heads + h], axis=1, keepdims=True)
        meet = meet * jax.nn.sigmoid(beta_in)
        read_q = read[h * rows : (h + 1) * rows]
        read_k = read[pairs + h * rows : pairs + (h + 1) * rows]
        readout = decay * read_q + meet * (v_all[:, lanes] - decay * read_k)
        outs.append(rms_scale(readout, head_gain_ref[...], 0.01).astype(BF))
    head_out = jnp.concatenate(outs, axis=1)
    get_out.wait()
    partial = dot32(head_out, out_w_ref[...]).astype(BF)
    for t in range(partial_ref.shape[0]):
        partial_ref[t] = partial


def mixer(hidden, state, gain, query, key, value, decay, beta, rate, head_gain, out_w, ids, n_ep, n_tp, near):
    rows, width = hidden.shape
    vmem = pl.BlockSpec(memory_space=pltpu.VMEM)
    smem = pl.BlockSpec(memory_space=pltpu.SMEM)
    hbm = pl.BlockSpec(memory_space=pl.ANY)
    state = state.reshape(-1, state.shape[-1])
    return pl.pallas_call(
        functools.partial(mixer_body, near),
        out_shape=(
            jax.ShapeDtypeStruct((n_tp, rows, width), BF),
            jax.ShapeDtypeStruct((n_ep * 8, 2 * rows), BF),
            jax.ShapeDtypeStruct(ids.shape, jnp.int32),
        ),
        in_specs=[vmem] * 4 + [smem, vmem, vmem] + [hbm] * 5,
        out_specs=(vmem,) * 3,
        scratch_shapes=[
            pltpu.VMEM(query.shape, BF),
            pltpu.VMEM(key.shape, BF),
            pltpu.VMEM(value.shape, BF),
            pltpu.VMEM(out_w.shape, BF),
            pltpu.VMEM(state.shape, F32),
            pltpu.SemaphoreType.DMA((8,)),
        ],
        name="mixer",
    )(
        hidden,
        gain[None],
        decay.T,
        beta.T,
        rate,
        head_gain[None],
        ids.T,
        query,
        key,
        value,
        out_w,
        state,
    )


def spread_body(*refs):
    sources, target = refs[:-1], refs[-1]
    rows = sources[0].shape[0]
    for w, source in enumerate(sources):
        for c in range(target.shape[0]):
            target[c, w * rows : (w + 1) * rows, :] = source[...]


def spread(weights, count):
    rows, width = weights[0].shape
    vmem = pl.BlockSpec(memory_space=pltpu.VMEM)
    return pl.pallas_call(
        spread_body,
        out_shape=jax.ShapeDtypeStruct((count, len(weights) * rows, width), BF),
        in_specs=[vmem] * len(weights),
        out_specs=vmem,
        name="spread",
    )(*weights)


def exchange(blocks, axis):
    return lax.all_to_all(blocks, axis, split_axis=0, concat_axis=0, tiled=True)


def local(
    hidden_in,
    prior_state,
    mix_gain,
    query_w,
    key_w,
    value_w,
    decay_w,
    beta_w,
    decay_rate,
    head_gain,
    out_w,
    ffn_gain,
    expert_ids,
    group_share,
    expert_share,
    expert_gate,
    expert_up,
    expert_down,
    dense_gate,
    dense_up,
    dense_down,
    branch_gate,
):
    rows, width = hidden_in.shape
    n_ep = lax.axis_size(EP)
    n_tp = lax.axis_size("x")
    n_near = lax.axis_size(NEAR)
    quarter = width // n_tp
    cap = 2
    per_near = rows // n_near
    tp_at = lax.axis_index("x")
    hid = dense_gate.shape[0]

    copies = spread((dense_gate, dense_up, dense_down), n_near)
    dense_near = exchange(copies, NEAR).reshape(n_near, 3, hid, quarter)

    copies_out, pick, position = mixer(
        hidden_in,
        prior_state,
        mix_gain,
        query_w,
        key_w,
        value_w,
        decay_w,
        beta_w,
        decay_rate,
        head_gain,
        out_w,
        expert_ids,
        n_ep,
        n_tp,
        n_near,
    )
    partials = exchange(copies_out, "x")
    mix = jnp.sum(partials.astype(F32), axis=0)
    resid = (hidden_in.astype(F32) + mix).astype(BF)
    normed2 = rms_scale(resid.astype(F32), ffn_gain, 0.1).astype(BF)
    own = lax.dynamic_slice_in_dim(normed2, tp_at * quarter, quarter, 1)
    resid_own = lax.dynamic_slice_in_dim(resid, tp_at * quarter, quarter, 1).astype(F32)
    branch_weight = jax.nn.sigmoid(dot32(normed2, branch_gate))[:, None]

    block = cap + per_near
    halves = jnp.concatenate([own[:, : quarter // 2], own[:, quarter // 2 :]], axis=0)
    sent = dot32(pick, halves).astype(BF)
    n_hid = n_near * hid
    gate_near = dense_near[:, 0].reshape(n_hid, quarter)
    up_near = dense_near[:, 1].reshape(n_hid, quarter)
    down_near = dense_near[:, 2].reshape(n_hid, quarter)
    route_weight = (
        group_share[:, None] * expert_share / jnp.sum(expert_share, axis=1, keepdims=True)
    )
    fetch = (position[:, :, None] == jnp.arange(n_ep * cap)).astype(BF)
    ready = (sent, gate_near, up_near, down_near, fetch, route_weight, branch_weight, resid_own)
    ready = lax.optimization_barrier(ready)
    sent, gate_near, up_near, down_near, fetch, route_weight, branch_weight, resid_own = ready
    arrived = exchange(sent.reshape(n_ep, 8, quarter // 2), EP)
    arrived = arrived.reshape(n_ep, 2, block, quarter // 2)
    arrived = jnp.concatenate([arrived[:, 0], arrived[:, 1]], axis=2)
    moe_rows = arrived[:, :cap].reshape(n_ep * cap, quarter)
    dense_rows = arrived[:, cap:].reshape(n_ep * per_near, quarter)

    contract = (((1,), (1,)), ((), ()))
    gate_part = lax.dot_general(dense_rows, gate_near, contract, preferred_element_type=F32)
    up_part = lax.dot_general(dense_rows, up_near, contract, preferred_element_type=F32)
    share = n_hid // n_tp
    pre = jnp.stack(
        [gate_part.reshape(-1, n_tp, share), up_part.reshape(-1, n_tp, share)], axis=2
    ).astype(BF)
    pre = jnp.moveaxis(pre, 1, 0).reshape(n_tp, -1, 2 * share)
    moe_copies = jnp.broadcast_to(moe_rows, (n_tp, *moe_rows.shape))
    first = exchange(jnp.concatenate([moe_copies, pre], axis=2), "x")

    full_rows = jnp.moveaxis(first[:, :, :quarter], 0, 1).reshape(n_ep * cap, width)
    pre_sum = jnp.sum(first[:, :, quarter:].astype(F32), axis=0)
    dense_hidden = (jax.nn.silu(pre_sum[:, :share]) * pre_sum[:, share:]).astype(BF)
    gate_pre = dot32(full_rows, expert_gate[0])
    up_pre = dot32(full_rows, expert_up[0])
    hidden = (jax.nn.silu(gate_pre) * up_pre).astype(BF)
    expert_part = dot32(hidden, expert_down[0]).astype(BF)
    part_blocks = jnp.moveaxis(expert_part.reshape(n_ep * cap, n_tp, quarter), 1, 0)
    hidden_copies = jnp.broadcast_to(dense_hidden, (n_tp, *dense_hidden.shape))
    second = exchange(jnp.concatenate([part_blocks, hidden_copies], axis=2), "x")

    expert_out = jnp.sum(second[:, :, :quarter].astype(F32), axis=0).astype(BF)
    all_hidden = jnp.moveaxis(second[:, :, quarter:], 0, 1).reshape(n_ep * per_near, n_hid)
    dense_out = dot32(all_hidden, down_near).astype(BF)
    back = jnp.concatenate(
        [expert_out.reshape(n_ep, cap, quarter), dense_out.reshape(n_ep, per_near, quarter)], axis=1
    )
    returned = exchange(back, EP)

    slots = returned[:, :cap].reshape(n_ep * cap, quarter)
    per_choice = dot32(fetch.reshape(rows * 2, n_ep * cap), slots).reshape(rows, 2, quarter)
    moe = jnp.sum(per_choice * route_weight[:, :, None], axis=1)
    sides = [lax.axis_size(axis) for axis in EP]
    branch = jnp.sum(
        returned[:, cap:].astype(F32).reshape(*sides, per_near, quarter), axis=(0, 2)
    ).reshape(rows, quarter)
    return (resid_own + moe + branch_weight * branch).astype(BF)


def solution(mesh):
    torus = Mesh(mesh.devices.reshape(4, 2, 4, 2, 2, mesh.shape["tp"]), (*EP, "x"))
    placed = (
        P(EP, None),
        P(EP, "x", None, None),
        P(),
        P(None, "x"),
        P(None, "x"),
        P(None, "x"),
        P(None, "x"),
        P(None, "x"),
        P("x"),
        P(),
        P("x", None),
        P(),
        P(EP, None),
        P(EP),
        P(EP, None),
        P(EP, None, "x"),
        P(EP, None, "x"),
        P(EP, "x", None),
        P(EP, "x"),
        P(EP, "x"),
        P(EP, "x"),
        P(),
    )
    return jax.shard_map(local, mesh=torus, in_specs=placed, out_specs=P(EP, "x"), check_vma=False)
```

```python
import functools

import jax
import jax.numpy as jnp
from jax import lax
from jax.experimental import pallas as pl
from jax.experimental.pallas import tpu as pltpu
from jax.sharding import Mesh
from jax.sharding import PartitionSpec as P

EP = ("z_hi", "z_lo", "y_hi", "y_lo", "c")
NEAR = ("z_lo", "y_lo", "c")
BF = jnp.bfloat16
F32 = jnp.float32


def rms_scale(values, gain, floor):
    return values * lax.rsqrt(jnp.mean(values * values, axis=-1, keepdims=True) + floor) * gain


def unit_rows(values):
    return values * lax.rsqrt(jnp.sum(values * values, axis=-1, keepdims=True) + 1.0)


def dot32(a, b):
    return jnp.dot(a, b, preferred_element_type=F32)


def slots_of(ids_ref, pick_ref, fetch_ref, near, rows):
    choices = ids_ref.shape[0]
    row_ids = ids_ref[...].astype(F32)
    r_at = lax.broadcasted_iota(jnp.int32, (rows, rows), 0)
    c_at = lax.broadcasted_iota(jnp.int32, (rows, rows), 1)
    eye = jnp.where(r_at == c_at, 1.0, 0.0)
    col_ids = lax.dot_general(eye, row_ids, (((1,), (1,)), ((), ())), preferred_element_type=F32)
    row_slots, col_slots = [], []
    for j in range(choices):
        by_row = jnp.zeros((rows, rows), F32)
        by_col = jnp.zeros((rows, rows), F32)
        for o in range(choices):
            by_row += jnp.where(col_ids[:, o : o + 1] == row_ids[j : j + 1, :], 1.0, 0.0)
            by_col += jnp.where(col_ids[:, j : j + 1] == row_ids[o : o + 1, :], 1.0, 0.0)
        row_rank = jnp.sum(jnp.where(r_at < c_at, by_row, 0.0), axis=0, keepdims=True)
        col_rank = jnp.sum(jnp.where(c_at < r_at, by_col, 0.0), axis=1, keepdims=True)
        row_slots.append(row_ids[j : j + 1, :] * 2.0 + row_rank)
        col_slots.append(col_ids[:, j : j + 1] * 2.0 + col_rank)
    place = lax.broadcasted_iota(jnp.int32, (rows, fetch_ref.shape[1]), 1).astype(F32)
    fetch_ref[...] = jnp.concatenate(
        [jnp.where(place == found, 1.0, 0.0) for found in col_slots], axis=0
    ).astype(BF)

    shape = (8, 2 * rows)
    at = lax.broadcasted_iota(jnp.int32, shape, 0)
    col = lax.broadcasted_iota(jnp.int32, shape, 1)
    slot = (at & 1).astype(F32)
    same_half = (at >= 4) == (col >= rows)
    for_expert = (at & 2) == 0
    token = jnp.where(col >= rows, col - rows, col).astype(F32)
    expert_keys = [
        jnp.where(
            same_half & for_expert, jnp.concatenate([found, found], axis=1) - slot, -1.0
        )
        for found in row_slots
    ]
    dense_key = jnp.where(same_half, jnp.where(for_expert, -1.0, token - slot), -1.0)
    dense_hit = [dense_key == 2.0 * n for n in range(near)]
    blocks = []
    for d in range(pick_ref.shape[0] // 8):
        hit = dense_hit[d // 16 % 2 * 4 + d // 2 % 2 * 2 + d % 2]
        for key in expert_keys:
            hit = hit | (key == 2.0 * d)
        blocks.append(jnp.where(hit, 1.0, 0.0))
    pick_ref[...] = jnp.concatenate(blocks, axis=0).astype(BF)


def mixer_body(near, *refs):
    rate_ref, sources, targets, buffers = refs[0], refs[1:12], refs[12:15], refs[15:29]
    sems = refs[29]
    (
        hidden_ref,
        gain_ref,
        decay_ref,
        beta_ref,
        head_gain_ref,
        ids_ref,
        query_ref,
        key_ref,
        value_ref,
        out_w_ref,
        state_ref,
        partial_ref,
        pick_ref,
        fetch_ref,
    ) = buffers
    rows = hidden_ref.shape[0]
    heads = decay_ref.shape[0]
    dv = head_gain_ref.shape[1]
    dk = query_ref.shape[1] // heads
    groups = 4
    step = state_ref.shape[0] // groups

    def copy_of(source, target, at):
        return pltpu.make_async_copy(source, target, sems.at[at])

    gets = [copy_of(sources[n], buffers[n], n) for n in range(10)]
    get_state = [
        copy_of(
            sources[10].at[pl.ds(g * step, step)], state_ref.at[pl.ds(g * step, step)], 10 + g
        )
        for g in range(groups)
    ]
    puts = [copy_of(buffers[11 + n], targets[n], 14 + n) for n in range(3)]
    for copy in gets[:8] + get_state + gets[8:]:
        copy.start()
    gets[5].wait()
    slots_of(ids_ref, pick_ref, fetch_ref, near, rows)
    puts[1].start()
    puts[2].start()
    for copy in gets[:5]:
        copy.wait()
    wide = hidden_ref[...].astype(F32)
    normed = rms_scale(wide, gain_ref[...], 0.1).astype(BF)
    wide = normed.astype(F32)
    gets[6].wait()
    q_all = dot32(normed, query_ref[...])
    gets[7].wait()
    k_all = dot32(normed, key_ref[...])
    units = []
    for source in (q_all, k_all):
        for h in range(heads):
            units.append(unit_rows(source[:, h * dk : (h + 1) * dk]))
    stacked = jnp.concatenate(units, axis=0).astype(BF)
    pairs = heads * rows
    row_at = lax.broadcasted_iota(jnp.int32, stacked.shape, 0) % pairs
    zero = jnp.zeros_like(stacked)
    read = jnp.zeros((2 * pairs, dv), F32)
    for g in range(groups):
        get_state[g].wait()
        blocks = []
        for b in range(g * step // dk, (g + 1) * step // dk):
            blocks.append(jnp.where(row_at == (b % heads) * rows + b // heads, stacked, zero))
        state = state_ref[g * step : (g + 1) * step].astype(BF)
        read = read + dot32(jnp.concatenate(blocks, axis=1), state)
    gets[8].wait()
    v_all = dot32(normed, value_ref[...])
    outs = []
    for h in range(heads):
        lanes = slice(h * dv, (h + 1) * dv)
        decay_in = jnp.sum(wide * decay_ref[h : h + 1, :].astype(F32), axis=1, keepdims=True)
        beta_in = jnp.sum(wide * beta_ref[h : h + 1, :].astype(F32), axis=1, keepdims=True)
        decay = jnp.exp(-rate_ref[h] * jax.nn.softplus(decay_in))
        meet = jnp.sum(units[h] * units[heads + h], axis=1, keepdims=True)
        meet = meet * jax.nn.sigmoid(beta_in)
        read_q = read[h * rows : (h + 1) * rows]
        read_k = read[pairs + h * rows : pairs + (h + 1) * rows]
        readout = decay * read_q + meet * (v_all[:, lanes] - decay * read_k)
        outs.append(rms_scale(readout, head_gain_ref[...], 0.01).astype(BF))
    head_out = jnp.concatenate(outs, axis=1)
    gets[9].wait()
    partial = dot32(head_out, out_w_ref[...]).astype(BF)
    for t in range(partial_ref.shape[0]):
        partial_ref[t] = partial
    puts[0].start()
    for copy in puts:
        copy.wait()


def mixer(hidden, state, gain, query, key, value, decay, beta, rate, head_gain, out_w, ids, n_ep, n_tp, near):
    rows, width = hidden.shape
    smem = pl.BlockSpec(memory_space=pltpu.SMEM)
    anywhere = pl.BlockSpec(memory_space=pl.ANY)
    arrays = (
        hidden,
        gain[None],
        decay.T,
        beta.T,
        head_gain[None],
        ids.T,
        query,
        key,
        value,
        out_w,
        state.reshape(-1, state.shape[-1]),
    )
    outs = (
        jax.ShapeDtypeStruct((n_tp, rows, width), BF),
        jax.ShapeDtypeStruct((n_ep * 8, 2 * rows), BF),
        jax.ShapeDtypeStruct((ids.size, 2 * n_ep), BF),
    )
    return pl.pallas_call(
        functools.partial(mixer_body, near),
        out_shape=outs,
        in_specs=[smem] + [anywhere] * len(arrays),
        out_specs=(anywhere,) * len(outs),
        scratch_shapes=[pltpu.VMEM(a.shape, a.dtype) for a in (*arrays, *outs)]
        + [pltpu.SemaphoreType.DMA((17,))],
        name="mixer",
    )(rate, *arrays)


def spread_body(*refs):
    sources, target = refs[:-1], refs[-1]
    rows = sources[0].shape[0]
    for w, source in enumerate(sources):
        for c in range(target.shape[0]):
            target[c, w * rows : (w + 1) * rows, :] = source[...]


def spread(weights, count):
    rows, width = weights[0].shape
    vmem = pl.BlockSpec(memory_space=pltpu.VMEM)
    return pl.pallas_call(
        spread_body,
        out_shape=jax.ShapeDtypeStruct((count, len(weights) * rows, width), BF),
        in_specs=[vmem] * len(weights),
        out_specs=vmem,
        name="spread",
    )(*weights)


def exchange(blocks, axis):
    return lax.all_to_all(blocks, axis, split_axis=0, concat_axis=0, tiled=True)


def local(
    hidden_in,
    prior_state,
    mix_gain,
    query_w,
    key_w,
    value_w,
    decay_w,
    beta_w,
    decay_rate,
    head_gain,
    out_w,
    ffn_gain,
    expert_ids,
    group_share,
    expert_share,
    expert_gate,
    expert_up,
    expert_down,
    dense_gate,
    dense_up,
    dense_down,
    branch_gate,
):
    rows, width = hidden_in.shape
    n_ep = lax.axis_size(EP)
    n_tp = lax.axis_size("x")
    n_near = lax.axis_size(NEAR)
    quarter = width // n_tp
    cap = 2
    per_near = rows // n_near
    tp_at = lax.axis_index("x")
    hid = dense_gate.shape[0]

    copies = spread((dense_gate, dense_up, dense_down), n_near)
    dense_near = exchange(copies, NEAR).reshape(n_near, 3, hid, quarter)

    copies_out, pick, fetch = mixer(
        hidden_in,
        prior_state,
        mix_gain,
        query_w,
        key_w,
        value_w,
        decay_w,
        beta_w,
        decay_rate,
        head_gain,
        out_w,
        expert_ids,
        n_ep,
        n_tp,
        n_near,
    )
    partials = exchange(copies_out, "x")
    mix = jnp.sum(partials.astype(F32), axis=0)
    resid = (hidden_in.astype(F32) + mix).astype(BF)
    normed2 = rms_scale(resid.astype(F32), ffn_gain, 0.1).astype(BF)
    own = lax.dynamic_slice_in_dim(normed2, tp_at * quarter, quarter, 1)
    resid_own = lax.dynamic_slice_in_dim(resid, tp_at * quarter, quarter, 1).astype(F32)
    gate_wide = branch_gate.astype(F32)
    branch_dot = jnp.sum(normed2.astype(F32) * gate_wide, axis=1, keepdims=True)
    branch_weight = jax.nn.sigmoid(branch_dot)

    block = cap + per_near
    halves = jnp.concatenate([own[:, : quarter // 2], own[:, quarter // 2 :]], axis=0)
    sent = dot32(pick, halves).astype(BF)
    n_hid = n_near * hid
    gate_near = dense_near[:, 0].reshape(n_hid, quarter)
    up_near = dense_near[:, 1].reshape(n_hid, quarter)
    down_near = dense_near[:, 2].reshape(n_hid, quarter)
    route_weight = (
        group_share[:, None] * expert_share / jnp.sum(expert_share, axis=1, keepdims=True)
    )
    first_weight, second_weight = route_weight[:, :1], route_weight[:, 1:]
    sent, gate_near, up_near, down_near, fetch = lax.optimization_barrier(
        (sent, gate_near, up_near, down_near, fetch)
    )
    sent, first_weight, second_weight, branch_weight, resid_own = lax.optimization_barrier(
        (sent, first_weight, second_weight, branch_weight, resid_own)
    )
    arrived = exchange(sent.reshape(n_ep, 8, quarter // 2), EP)
    arrived = arrived.reshape(n_ep, 2, block, quarter // 2)
    arrived = jnp.concatenate([arrived[:, 0], arrived[:, 1]], axis=2)
    moe_rows = arrived[:, :cap].reshape(n_ep * cap, quarter)
    dense_rows = arrived[:, cap:].reshape(n_ep * per_near, quarter)

    contract = (((1,), (1,)), ((), ()))
    gate_part = lax.dot_general(dense_rows, gate_near, contract, preferred_element_type=F32)
    up_part = lax.dot_general(dense_rows, up_near, contract, preferred_element_type=F32)
    share = n_hid // n_tp
    pre = jnp.stack(
        [gate_part.reshape(-1, n_tp, share), up_part.reshape(-1, n_tp, share)], axis=2
    ).astype(BF)
    pre = jnp.moveaxis(pre, 1, 0).reshape(n_tp, -1, 2 * share)
    moe_copies = jnp.broadcast_to(moe_rows, (n_tp, *moe_rows.shape))
    first = exchange(jnp.concatenate([moe_copies, pre], axis=2), "x")

    full_rows = jnp.moveaxis(first[:, :, :quarter], 0, 1).reshape(n_ep * cap, width)
    pre_sum = jnp.sum(first[:, :, quarter:].astype(F32), axis=0)
    dense_hidden = (jax.nn.silu(pre_sum[:, :share]) * pre_sum[:, share:]).astype(BF)
    gate_pre = dot32(full_rows, expert_gate[0])
    up_pre = dot32(full_rows, expert_up[0])
    hidden = (jax.nn.silu(gate_pre) * up_pre).astype(BF)
    expert_part = dot32(hidden, expert_down[0]).astype(BF)
    part_blocks = jnp.moveaxis(expert_part.reshape(n_ep * cap, n_tp, quarter), 1, 0)
    hidden_copies = jnp.broadcast_to(dense_hidden, (n_tp, *dense_hidden.shape))
    second = exchange(jnp.concatenate([part_blocks, hidden_copies], axis=2), "x")

    expert_out = jnp.sum(second[:, :, :quarter].astype(F32), axis=0).astype(BF)
    all_hidden = jnp.moveaxis(second[:, :, quarter:], 0, 1).reshape(n_ep * per_near, n_hid)
    dense_out = dot32(all_hidden, down_near).astype(BF)
    back = jnp.concatenate(
        [expert_out.reshape(n_ep, cap, quarter), dense_out.reshape(n_ep, per_near, quarter)], axis=1
    )
    returned = exchange(back, EP)

    slots = returned[:, :cap].reshape(n_ep * cap, quarter)
    per_choice = dot32(fetch, slots)
    moe = per_choice[:rows] * first_weight + per_choice[rows:] * second_weight
    sides = [lax.axis_size(axis) for axis in EP]
    branch = jnp.sum(
        returned[:, cap:].astype(F32).reshape(*sides, per_near, quarter), axis=(0, 2)
    ).reshape(rows, quarter)
    return (resid_own + moe + branch_weight * branch).astype(BF)


def solution(mesh):
    torus = Mesh(mesh.devices.reshape(4, 2, 4, 2, 2, mesh.shape["tp"]), (*EP, "x"))
    placed = (
        P(EP, None),
        P(EP, "x", None, None),
        P(),
        P(None, "x"),
        P(None, "x"),
        P(None, "x"),
        P(None, "x"),
        P(None, "x"),
        P("x"),
        P(),
        P("x", None),
        P(),
        P(EP, None),
        P(EP),
        P(EP, None),
        P(EP, None, "x"),
        P(EP, None, "x"),
        P(EP, "x", None),
        P(EP, "x"),
        P(EP, "x"),
        P(EP, "x"),
        P(),
    )
    return jax.shard_map(local, mesh=torus, in_specs=placed, out_specs=P(EP, "x"), check_vma=False)
```

```python
import functools

import jax
import jax.numpy as jnp
from jax import lax
from jax.experimental import pallas as pl
from jax.experimental.pallas import tpu as pltpu
from jax.sharding import Mesh
from jax.sharding import PartitionSpec as P

EP = ("z_hi", "z_lo", "y_hi", "y_lo", "c")
NEAR = ("z_lo", "y_lo", "c")
BF = jnp.bfloat16
F32 = jnp.float32


def rms_scale(values, gain, floor):
    return values * lax.rsqrt(jnp.mean(values * values, axis=-1, keepdims=True) + floor) * gain


def unit_rows(values):
    return values * lax.rsqrt(jnp.sum(values * values, axis=-1, keepdims=True) + 1.0)


def dot32(a, b):
    return jnp.dot(a, b, preferred_element_type=F32)


def slots_of(ids_ref, pick_ref, fetch_ref, near, rows):
    choices = ids_ref.shape[0]
    row_ids = ids_ref[...].astype(F32)
    r_at = lax.broadcasted_iota(jnp.int32, (rows, rows), 0)
    c_at = lax.broadcasted_iota(jnp.int32, (rows, rows), 1)
    eye = jnp.where(r_at == c_at, 1.0, 0.0)
    col_ids = lax.dot_general(eye, row_ids, (((1,), (1,)), ((), ())), preferred_element_type=F32)
    row_slots, col_slots = [], []
    for j in range(choices):
        by_row = jnp.zeros((rows, rows), F32)
        by_col = jnp.zeros((rows, rows), F32)
        for o in range(choices):
            by_row += jnp.where(col_ids[:, o : o + 1] == row_ids[j : j + 1, :], 1.0, 0.0)
            by_col += jnp.where(col_ids[:, j : j + 1] == row_ids[o : o + 1, :], 1.0, 0.0)
        row_rank = jnp.sum(jnp.where(r_at < c_at, by_row, 0.0), axis=0, keepdims=True)
        col_rank = jnp.sum(jnp.where(c_at < r_at, by_col, 0.0), axis=1, keepdims=True)
        row_slots.append(row_ids[j : j + 1, :] * 2.0 + row_rank)
        col_slots.append(col_ids[:, j : j + 1] * 2.0 + col_rank)
    place = lax.broadcasted_iota(jnp.int32, (rows, fetch_ref.shape[1]), 1).astype(F32)
    fetch_ref[...] = jnp.concatenate(
        [jnp.where(place == found, 1.0, 0.0) for found in col_slots], axis=0
    ).astype(BF)

    shape = (8, 2 * rows)
    at = lax.broadcasted_iota(jnp.int32, shape, 0)
    col = lax.broadcasted_iota(jnp.int32, shape, 1)
    slot = (at & 1).astype(F32)
    same_half = (at >= 4) == (col >= rows)
    for_expert = (at & 2) == 0
    token = jnp.where(col >= rows, col - rows, col).astype(F32)
    expert_keys = [
        jnp.where(
            same_half & for_expert, jnp.concatenate([found, found], axis=1) - slot, -1.0
        )
        for found in row_slots
    ]
    dense_key = jnp.where(same_half, jnp.where(for_expert, -1.0, token - slot), -1.0)
    dense_hit = [dense_key == 2.0 * n for n in range(near)]
    blocks = []
    for d in range(pick_ref.shape[0] // 8):
        hit = dense_hit[d // 16 % 2 * 4 + d // 2 % 2 * 2 + d % 2]
        for key in expert_keys:
            hit = hit | (key == 2.0 * d)
        blocks.append(jnp.where(hit, 1.0, 0.0))
    pick_ref[...] = jnp.concatenate(blocks, axis=0).astype(BF)


def mixer_body(near, *refs):
    rate_ref, sources, targets, buffers = refs[0], refs[1:12], refs[12:15], refs[15:29]
    sems = refs[29]
    (
        hidden_ref,
        gain_ref,
        decay_ref,
        beta_ref,
        head_gain_ref,
        ids_ref,
        query_ref,
        key_ref,
        value_ref,
        out_w_ref,
        state_ref,
        partial_ref,
        pick_ref,
        fetch_ref,
    ) = buffers
    rows = hidden_ref.shape[0]
    heads = decay_ref.shape[0]
    dv = head_gain_ref.shape[1]
    dk = query_ref.shape[1] // heads
    groups = 4
    step = state_ref.shape[0] // groups

    def copy_of(source, target, at):
        return pltpu.make_async_copy(source, target, sems.at[at])

    gets = [copy_of(sources[n], buffers[n], n) for n in range(10)]
    get_state = [
        copy_of(
            sources[10].at[pl.ds(g * step, step)], state_ref.at[pl.ds(g * step, step)], 10 + g
        )
        for g in range(groups)
    ]
    puts = [copy_of(buffers[11 + n], targets[n], 14 + n) for n in range(3)]
    for copy in gets[:8] + get_state + gets[8:]:
        copy.start()
    gets[5].wait()
    slots_of(ids_ref, pick_ref, fetch_ref, near, rows)
    puts[1].start()
    puts[2].start()
    for copy in gets[:5]:
        copy.wait()
    wide = hidden_ref[...].astype(F32)
    normed = rms_scale(wide, gain_ref[...], 0.1).astype(BF)
    wide = normed.astype(F32)
    gets[6].wait()
    q_all = dot32(normed, query_ref[...])
    gets[7].wait()
    k_all = dot32(normed, key_ref[...])
    units = []
    for source in (q_all, k_all):
        for h in range(heads):
            units.append(unit_rows(source[:, h * dk : (h + 1) * dk]))
    stacked = jnp.concatenate(units, axis=0).astype(BF)
    pairs = heads * rows
    row_at = lax.broadcasted_iota(jnp.int32, stacked.shape, 0) % pairs
    zero = jnp.zeros_like(stacked)
    read = jnp.zeros((2 * pairs, dv), F32)
    for g in range(groups):
        get_state[g].wait()
        blocks = []
        for b in range(g * step // dk, (g + 1) * step // dk):
            blocks.append(jnp.where(row_at == (b % heads) * rows + b // heads, stacked, zero))
        state = state_ref[g * step : (g + 1) * step].astype(BF)
        read = read + dot32(jnp.concatenate(blocks, axis=1), state)
    gets[8].wait()
    v_all = dot32(normed, value_ref[...])
    outs = []
    for h in range(heads):
        lanes = slice(h * dv, (h + 1) * dv)
        decay_in = jnp.sum(wide * decay_ref[h : h + 1, :].astype(F32), axis=1, keepdims=True)
        beta_in = jnp.sum(wide * beta_ref[h : h + 1, :].astype(F32), axis=1, keepdims=True)
        decay = jnp.exp(-rate_ref[h] * jax.nn.softplus(decay_in))
        meet = jnp.sum(units[h] * units[heads + h], axis=1, keepdims=True)
        meet = meet * jax.nn.sigmoid(beta_in)
        read_q = read[h * rows : (h + 1) * rows]
        read_k = read[pairs + h * rows : pairs + (h + 1) * rows]
        readout = decay * read_q + meet * (v_all[:, lanes] - decay * read_k)
        outs.append(rms_scale(readout, head_gain_ref[...], 0.01).astype(BF))
    head_out = jnp.concatenate(outs, axis=1)
    gets[9].wait()
    partial = dot32(head_out, out_w_ref[...]).astype(BF)
    for t in range(partial_ref.shape[0]):
        partial_ref[t] = partial
    puts[0].start()
    for copy in puts:
        copy.wait()


def mixer(hidden, state, gain, query, key, value, decay, beta, rate, head_gain, out_w, ids, n_ep, n_tp, near):
    rows, width = hidden.shape
    smem = pl.BlockSpec(memory_space=pltpu.SMEM)
    anywhere = pl.BlockSpec(memory_space=pl.ANY)
    arrays = (
        hidden,
        gain[None],
        decay.T,
        beta.T,
        head_gain[None],
        ids.T,
        query,
        key,
        value,
        out_w,
        state.reshape(-1, state.shape[-1]),
    )
    outs = (
        jax.ShapeDtypeStruct((n_tp, rows, width), BF),
        jax.ShapeDtypeStruct((n_ep * 8, 2 * rows), BF),
        jax.ShapeDtypeStruct((ids.size, 2 * n_ep), BF),
    )
    return pl.pallas_call(
        functools.partial(mixer_body, near),
        out_shape=outs,
        in_specs=[smem] + [anywhere] * len(arrays),
        out_specs=(anywhere,) * len(outs),
        scratch_shapes=[pltpu.VMEM(a.shape, a.dtype) for a in (*arrays, *outs)]
        + [pltpu.SemaphoreType.DMA((17,))],
        name="mixer",
    )(rate, *arrays)


def spread_body(*refs):
    sources, target = refs[:-1], refs[-1]
    rows = sources[0].shape[0]
    for w, source in enumerate(sources):
        for c in range(target.shape[0]):
            target[c, w * rows : (w + 1) * rows, :] = source[...]


def spread(weights, count):
    rows, width = weights[0].shape
    vmem = pl.BlockSpec(memory_space=pltpu.VMEM)
    return pl.pallas_call(
        spread_body,
        out_shape=jax.ShapeDtypeStruct((count, len(weights) * rows, width), BF),
        in_specs=[vmem] * len(weights),
        out_specs=vmem,
        name="spread",
    )(*weights)


def exchange(blocks, axis):
    return lax.all_to_all(blocks, axis, split_axis=0, concat_axis=0, tiled=True)


def local(
    hidden_in,
    prior_state,
    mix_gain,
    query_w,
    key_w,
    value_w,
    decay_w,
    beta_w,
    decay_rate,
    head_gain,
    out_w,
    ffn_gain,
    expert_ids,
    group_share,
    expert_share,
    expert_gate,
    expert_up,
    expert_down,
    dense_gate,
    dense_up,
    dense_down,
    branch_gate,
):
    rows, width = hidden_in.shape
    n_ep = lax.axis_size(EP)
    n_tp = lax.axis_size("x")
    n_near = lax.axis_size(NEAR)
    quarter = width // n_tp
    cap = 2
    per_near = rows // n_near
    tp_at = lax.axis_index("x")
    hid = dense_gate.shape[0]

    copies = spread((dense_gate, dense_up, dense_down), n_near)
    dense_near = exchange(copies, NEAR).reshape(n_near, 3, hid, quarter)

    copies_out, pick, fetch = mixer(
        hidden_in,
        prior_state,
        mix_gain,
        query_w,
        key_w,
        value_w,
        decay_w,
        beta_w,
        decay_rate,
        head_gain,
        out_w,
        expert_ids,
        n_ep,
        n_tp,
        n_near,
    )
    partials = exchange(copies_out, "x")
    mix = jnp.sum(partials.astype(F32), axis=0)
    resid = (hidden_in.astype(F32) + mix).astype(BF)
    normed2 = rms_scale(resid.astype(F32), ffn_gain, 0.1).astype(BF)
    own = lax.dynamic_slice_in_dim(normed2, tp_at * quarter, quarter, 1)
    resid_own = lax.dynamic_slice_in_dim(resid, tp_at * quarter, quarter, 1).astype(F32)
    gate_wide = branch_gate.astype(F32)
    branch_dot = jnp.sum(normed2.astype(F32) * gate_wide, axis=1, keepdims=True)
    branch_weight = jax.nn.sigmoid(branch_dot)

    block = cap + per_near
    halves = jnp.concatenate([own[:, : quarter // 2], own[:, quarter // 2 :]], axis=0)
    sent = dot32(pick, halves).astype(BF)
    n_hid = n_near * hid
    share = n_hid // n_tp
    pairs_near = dense_near[:, :2].reshape(n_tp, -1, 2, hid, quarter)
    both_near = jnp.swapaxes(pairs_near, 1, 2).reshape(2 * n_hid, quarter)
    down_near = dense_near[:, 2].reshape(n_hid, quarter)
    expert_both = jnp.concatenate([expert_gate[0], expert_up[0]], axis=1)
    route_weight = (
        group_share[:, None] * expert_share / jnp.sum(expert_share, axis=1, keepdims=True)
    )
    first_weight, second_weight = route_weight[:, :1], route_weight[:, 1:]
    sent, both_near, down_near, fetch, expert_both = lax.optimization_barrier(
        (sent, both_near, down_near, fetch, expert_both)
    )
    sent, first_weight, second_weight, branch_weight, resid_own = lax.optimization_barrier(
        (sent, first_weight, second_weight, branch_weight, resid_own)
    )
    arrived = exchange(sent.reshape(n_ep, 8, quarter // 2), EP)
    arrived = arrived.reshape(n_ep, 2, block, quarter // 2)
    arrived = jnp.concatenate([arrived[:, 0], arrived[:, 1]], axis=2)
    moe_rows = arrived[:, :cap].reshape(n_ep * cap, quarter)
    dense_rows = arrived[:, cap:].reshape(n_ep * per_near, quarter)

    contract = (((1,), (1,)), ((), ()))
    pre = lax.dot_general(both_near, dense_rows, contract, preferred_element_type=F32)
    pre = pre.astype(BF).reshape(n_tp, 2 * share, -1)
    moe_copies = jnp.broadcast_to(moe_rows, (n_tp, *moe_rows.shape))
    first = exchange(jnp.concatenate([moe_copies, pre], axis=1), "x")

    n_rows = n_ep * cap
    pre_sum = jnp.sum(first[:, n_rows:].astype(F32), axis=0)
    dense_hidden = (jax.nn.silu(pre_sum[:share]) * pre_sum[share:]).astype(BF)
    full_rows = jnp.concatenate([first[t, :n_rows] for t in range(n_tp)], axis=1)
    both_pre = dot32(full_rows, expert_both)
    wide = both_pre.shape[1] // 2
    hidden = (jax.nn.silu(both_pre[:, :wide]) * both_pre[:, wide:]).astype(BF)
    expert_part = dot32(hidden, expert_down[0]).astype(BF)
    part_blocks = jnp.stack(
        [expert_part[:, t * quarter : (t + 1) * quarter] for t in range(n_tp)], axis=0
    )
    hidden_copies = jnp.broadcast_to(dense_hidden, (n_tp, *dense_hidden.shape))
    second = exchange(jnp.concatenate([part_blocks, hidden_copies], axis=1), "x")

    expert_out = jnp.sum(second[:, :n_rows].astype(F32), axis=0).astype(BF)
    all_hidden = second[:, n_rows:].reshape(n_hid, -1)
    dense_out = lax.dot_general(
        all_hidden, down_near, (((0,), (0,)), ((), ())), preferred_element_type=F32
    ).astype(BF)
    back = jnp.concatenate(
        [expert_out.reshape(n_ep, cap, quarter), dense_out.reshape(n_ep, per_near, quarter)], axis=1
    )
    returned = exchange(back, EP)

    slots = returned[:, :cap].reshape(n_ep * cap, quarter)
    per_choice = dot32(fetch, slots)
    moe = per_choice[:rows] * first_weight + per_choice[rows:] * second_weight
    sides = [lax.axis_size(axis) for axis in EP]
    branch = jnp.sum(
        returned[:, cap:].astype(F32).reshape(*sides, per_near, quarter), axis=(0, 2)
    ).reshape(rows, quarter)
    return (resid_own + moe + branch_weight * branch).astype(BF)


def solution(mesh):
    torus = Mesh(mesh.devices.reshape(4, 2, 4, 2, 2, mesh.shape["tp"]), (*EP, "x"))
    placed = (
        P(EP, None),
        P(EP, "x", None, None),
        P(),
        P(None, "x"),
        P(None, "x"),
        P(None, "x"),
        P(None, "x"),
        P(None, "x"),
        P("x"),
        P(),
        P("x", None),
        P(),
        P(EP, None),
        P(EP),
        P(EP, None),
        P(EP, None, "x"),
        P(EP, None, "x"),
        P(EP, "x", None),
        P(EP, "x"),
        P(EP, "x"),
        P(EP, "x"),
        P(),
    )
    return jax.shard_map(local, mesh=torus, in_specs=placed, out_specs=P(EP, "x"), check_vma=False)
```

```python
import functools

import jax
import jax.numpy as jnp
from jax import lax
from jax.experimental import pallas as pl
from jax.experimental.pallas import tpu as pltpu
from jax.sharding import Mesh
from jax.sharding import PartitionSpec as P

EP = ("z_hi", "z_lo", "y_hi", "y_lo", "c")
NEAR = ("z_lo", "y_lo", "c")
BF = jnp.bfloat16
F32 = jnp.float32


def rms_scale(values, gain, floor):
    return values * lax.rsqrt(jnp.mean(values * values, axis=-1, keepdims=True) + floor) * gain


def unit_rows(values):
    return values * lax.rsqrt(jnp.sum(values * values, axis=-1, keepdims=True) + 1.0)


def dot32(a, b):
    return jnp.dot(a, b, preferred_element_type=F32)


def slots_of(ids_ref, pick_ref, fetch_ref, near, rows):
    choices = ids_ref.shape[0]
    row_ids = ids_ref[...].astype(F32)
    r_at = lax.broadcasted_iota(jnp.int32, (rows, rows), 0)
    c_at = lax.broadcasted_iota(jnp.int32, (rows, rows), 1)
    eye = jnp.where(r_at == c_at, 1.0, 0.0)
    col_ids = lax.dot_general(eye, row_ids, (((1,), (1,)), ((), ())), preferred_element_type=F32)
    row_slots, col_slots = [], []
    for j in range(choices):
        by_row = jnp.zeros((rows, rows), F32)
        by_col = jnp.zeros((rows, rows), F32)
        for o in range(choices):
            by_row += jnp.where(col_ids[:, o : o + 1] == row_ids[j : j + 1, :], 1.0, 0.0)
            by_col += jnp.where(col_ids[:, j : j + 1] == row_ids[o : o + 1, :], 1.0, 0.0)
        row_rank = jnp.sum(jnp.where(r_at < c_at, by_row, 0.0), axis=0, keepdims=True)
        col_rank = jnp.sum(jnp.where(c_at < r_at, by_col, 0.0), axis=1, keepdims=True)
        row_slots.append(row_ids[j : j + 1, :] * 2.0 + row_rank)
        col_slots.append(col_ids[:, j : j + 1] * 2.0 + col_rank)
    place = lax.broadcasted_iota(jnp.int32, (rows, fetch_ref.shape[1]), 1).astype(F32)
    fetch_ref[...] = jnp.concatenate(
        [jnp.where(place == found, 1.0, 0.0) for found in col_slots], axis=0
    ).astype(BF)

    shape = (8, 2 * rows)
    at = lax.broadcasted_iota(jnp.int32, shape, 0)
    col = lax.broadcasted_iota(jnp.int32, shape, 1)
    slot = (at & 1).astype(F32)
    same_half = (at >= 4) == (col >= rows)
    for_expert = (at & 2) == 0
    token = jnp.where(col >= rows, col - rows, col).astype(F32)
    expert_keys = [
        jnp.where(
            same_half & for_expert, jnp.concatenate([found, found], axis=1) - slot, -1.0
        )
        for found in row_slots
    ]
    dense_key = jnp.where(same_half, jnp.where(for_expert, -1.0, token - slot), -1.0)
    dense_hit = [dense_key == 2.0 * n for n in range(near)]
    blocks = []
    for d in range(pick_ref.shape[0] // 8):
        hit = dense_hit[d // 16 % 2 * 4 + d // 2 % 2 * 2 + d % 2]
        for key in expert_keys:
            hit = hit | (key == 2.0 * d)
        blocks.append(jnp.where(hit, 1.0, 0.0))
    pick_ref[...] = jnp.concatenate(blocks, axis=0).astype(BF)


def mixer_body(near, *refs):
    rate_ref, sources, targets, buffers = refs[0], refs[1:12], refs[12:15], refs[15:26]
    sems = refs[26]
    partial_ref, pick_ref, fetch_ref = targets
    (
        hidden_ref,
        gain_ref,
        decay_ref,
        beta_ref,
        head_gain_ref,
        ids_ref,
        query_ref,
        key_ref,
        value_ref,
        out_w_ref,
        state_ref,
    ) = buffers
    rows = hidden_ref.shape[0]
    heads = decay_ref.shape[0]
    dv = head_gain_ref.shape[1]
    dk = query_ref.shape[1] // heads
    groups = 4
    step = state_ref.shape[0] // groups

    def copy_of(source, target, at):
        return pltpu.make_async_copy(source, target, sems.at[at])

    gets = [copy_of(sources[n], buffers[n], n) for n in range(10)]
    get_state = [
        copy_of(
            sources[10].at[pl.ds(g * step, step)], state_ref.at[pl.ds(g * step, step)], 10 + g
        )
        for g in range(groups)
    ]
    for copy in gets[:8] + get_state + gets[8:]:
        copy.start()
    gets[5].wait()
    slots_of(ids_ref, pick_ref, fetch_ref, near, rows)
    for copy in gets[:5]:
        copy.wait()
    wide = hidden_ref[...].astype(F32)
    normed = rms_scale(wide, gain_ref[...], 0.1).astype(BF)
    wide = normed.astype(F32)
    gets[6].wait()
    q_all = dot32(normed, query_ref[...])
    gets[7].wait()
    k_all = dot32(normed, key_ref[...])
    units = []
    for source in (q_all, k_all):
        for h in range(heads):
            units.append(unit_rows(source[:, h * dk : (h + 1) * dk]))
    stacked = jnp.concatenate(units, axis=0).astype(BF)
    pairs = heads * rows
    row_at = lax.broadcasted_iota(jnp.int32, stacked.shape, 0) % pairs
    zero = jnp.zeros_like(stacked)
    read = jnp.zeros((2 * pairs, dv), F32)
    for g in range(groups):
        get_state[g].wait()
        blocks = []
        for b in range(g * step // dk, (g + 1) * step // dk):
            blocks.append(jnp.where(row_at == (b % heads) * rows + b // heads, stacked, zero))
        state = state_ref[g * step : (g + 1) * step].astype(BF)
        read = read + dot32(jnp.concatenate(blocks, axis=1), state)
    gets[8].wait()
    v_all = dot32(normed, value_ref[...])
    outs = []
    for h in range(heads):
        lanes = slice(h * dv, (h + 1) * dv)
        decay_in = jnp.sum(wide * decay_ref[h : h + 1, :].astype(F32), axis=1, keepdims=True)
        beta_in = jnp.sum(wide * beta_ref[h : h + 1, :].astype(F32), axis=1, keepdims=True)
        decay = jnp.exp(-rate_ref[h] * jax.nn.softplus(decay_in))
        meet = jnp.sum(units[h] * units[heads + h], axis=1, keepdims=True)
        meet = meet * jax.nn.sigmoid(beta_in)
        read_q = read[h * rows : (h + 1) * rows]
        read_k = read[pairs + h * rows : pairs + (h + 1) * rows]
        readout = decay * read_q + meet * (v_all[:, lanes] - decay * read_k)
        outs.append(rms_scale(readout, head_gain_ref[...], 0.01).astype(BF))
    head_out = jnp.concatenate(outs, axis=1)
    gets[9].wait()
    partial = dot32(head_out, out_w_ref[...]).astype(BF)
    for t in range(partial_ref.shape[0]):
        partial_ref[t] = partial


def mixer(hidden, state, gain, query, key, value, decay, beta, rate, head_gain, out_w, ids, n_ep, n_tp, near):
    rows, width = hidden.shape
    smem = pl.BlockSpec(memory_space=pltpu.SMEM)
    anywhere = pl.BlockSpec(memory_space=pl.ANY)
    arrays = (
        hidden,
        gain[None],
        decay.T,
        beta.T,
        head_gain[None],
        ids.T,
        query,
        key,
        value,
        out_w,
        state.reshape(-1, state.shape[-1]),
    )
    outs = (
        pltpu.VMEM((n_tp, rows, width), BF),
        pltpu.VMEM((n_ep * 8, 2 * rows), BF),
        pltpu.VMEM((ids.size, 2 * n_ep), BF),
    )
    return pl.pallas_call(
        functools.partial(mixer_body, near),
        out_shape=outs,
        in_specs=[smem] + [anywhere] * len(arrays),
        out_specs=(pl.BlockSpec(memory_space=pltpu.VMEM),) * len(outs),
        scratch_shapes=[pltpu.VMEM(a.shape, a.dtype) for a in arrays]
        + [pltpu.SemaphoreType.DMA((14,))],
        name="mixer",
    )(rate, *arrays)


def spread_body(*refs):
    sources, target = refs[:-1], refs[-1]
    rows = sources[0].shape[0]
    for w, source in enumerate(sources):
        for c in range(target.shape[0]):
            target[c, w * rows : (w + 1) * rows, :] = source[...]


def spread(weights, count):
    rows, width = weights[0].shape
    vmem = pl.BlockSpec(memory_space=pltpu.VMEM)
    return pl.pallas_call(
        spread_body,
        out_shape=jax.ShapeDtypeStruct((count, len(weights) * rows, width), BF),
        in_specs=[vmem] * len(weights),
        out_specs=vmem,
        name="spread",
    )(*weights)


def exchange(blocks, axis):
    return lax.all_to_all(blocks, axis, split_axis=0, concat_axis=0, tiled=True)


def local(
    hidden_in,
    prior_state,
    mix_gain,
    query_w,
    key_w,
    value_w,
    decay_w,
    beta_w,
    decay_rate,
    head_gain,
    out_w,
    ffn_gain,
    expert_ids,
    group_share,
    expert_share,
    expert_gate,
    expert_up,
    expert_down,
    dense_gate,
    dense_up,
    dense_down,
    branch_gate,
):
    rows, width = hidden_in.shape
    n_ep = lax.axis_size(EP)
    n_tp = lax.axis_size("x")
    n_near = lax.axis_size(NEAR)
    quarter = width // n_tp
    cap = 2
    per_near = rows // n_near
    tp_at = lax.axis_index("x")
    hid = dense_gate.shape[0]

    copies = spread((dense_gate, dense_up, dense_down), n_near)
    dense_near = exchange(copies, NEAR).reshape(n_near, 3, hid, quarter)

    copies_out, pick, fetch = mixer(
        hidden_in,
        prior_state,
        mix_gain,
        query_w,
        key_w,
        value_w,
        decay_w,
        beta_w,
        decay_rate,
        head_gain,
        out_w,
        expert_ids,
        n_ep,
        n_tp,
        n_near,
    )
    fetch, group_share, expert_share, expert_gate, expert_up, branch_gate, tp_at = (
        lax.optimization_barrier(
            (fetch, group_share, expert_share, expert_gate, expert_up, branch_gate, tp_at)
        )
    )
    n_hid = n_near * hid
    share = n_hid // n_tp
    pairs_near = dense_near[:, :2].reshape(n_tp, -1, 2, hid, quarter)
    both_near = jnp.swapaxes(pairs_near, 1, 2).reshape(2 * n_hid, quarter)
    down_near = dense_near[:, 2].reshape(n_hid, quarter)
    expert_both = jnp.concatenate([expert_gate[0], expert_up[0]], axis=1)
    route_weight = (
        group_share[:, None] * expert_share / jnp.sum(expert_share, axis=1, keepdims=True)
    )
    first_weight, second_weight = route_weight[:, :1], route_weight[:, 1:]
    gate_wide = branch_gate.astype(F32)
    half = quarter // 2
    offset, offset_half = tp_at * quarter, tp_at * quarter + half
    copies_out, both_near, down_near, fetch, offset, offset_half = lax.optimization_barrier(
        (copies_out, both_near, down_near, fetch, offset, offset_half)
    )
    copies_out, expert_both, first_weight, second_weight, gate_wide = lax.optimization_barrier(
        (copies_out, expert_both, first_weight, second_weight, gate_wide)
    )
    partials = exchange(copies_out, "x")
    mix = jnp.sum(partials.astype(F32), axis=0)
    resid = (hidden_in.astype(F32) + mix).astype(BF)
    normed2 = rms_scale(resid.astype(F32), ffn_gain, 0.1).astype(BF)
    resid_own = lax.dynamic_slice_in_dim(
        resid, offset, quarter, 1, allow_negative_indices=False
    ).astype(F32)
    branch_dot = jnp.sum(normed2.astype(F32) * gate_wide, axis=1, keepdims=True)
    branch_weight = jax.nn.sigmoid(branch_dot)

    block = cap + per_near
    halves = jnp.concatenate(
        [
            lax.dynamic_slice_in_dim(normed2, start, half, 1, allow_negative_indices=False)
            for start in (offset, offset_half)
        ],
        axis=0,
    )
    sent = dot32(pick, halves).astype(BF)
    sent, branch_weight, resid_own = lax.optimization_barrier((sent, branch_weight, resid_own))
    arrived = exchange(sent.reshape(n_ep, 8, quarter // 2), EP)
    arrived = arrived.reshape(n_ep, 2, block, quarter // 2)
    arrived = jnp.concatenate([arrived[:, 0], arrived[:, 1]], axis=2)
    moe_rows = arrived[:, :cap].reshape(n_ep * cap, quarter)
    dense_rows = arrived[:, cap:].reshape(n_ep * per_near, quarter)

    contract = (((1,), (1,)), ((), ()))
    pre = lax.dot_general(both_near, dense_rows, contract, preferred_element_type=F32)
    pre = pre.astype(BF).reshape(n_tp, 2 * share, -1)
    moe_copies = jnp.broadcast_to(moe_rows, (n_tp, *moe_rows.shape))
    first = exchange(jnp.concatenate([moe_copies, pre], axis=1), "x")

    n_rows = n_ep * cap
    pre_sum = jnp.sum(first[:, n_rows:].astype(F32), axis=0)
    dense_hidden = (jax.nn.silu(pre_sum[:share]) * pre_sum[share:]).astype(BF)
    full_rows = jnp.concatenate([first[t, :n_rows] for t in range(n_tp)], axis=1)
    both_pre = dot32(full_rows, expert_both)
    wide = both_pre.shape[1] // 2
    hidden = (jax.nn.silu(both_pre[:, :wide]) * both_pre[:, wide:]).astype(BF)
    expert_part = dot32(hidden, expert_down[0]).astype(BF)
    part_blocks = jnp.stack(
        [expert_part[:, t * quarter : (t + 1) * quarter] for t in range(n_tp)], axis=0
    )
    hidden_copies = jnp.broadcast_to(dense_hidden, (n_tp, *dense_hidden.shape))
    second = exchange(jnp.concatenate([part_blocks, hidden_copies], axis=1), "x")

    expert_out = jnp.sum(second[:, :n_rows].astype(F32), axis=0).astype(BF)
    all_hidden = second[:, n_rows:].reshape(n_hid, -1)
    dense_out = lax.dot_general(
        all_hidden, down_near, (((0,), (0,)), ((), ())), preferred_element_type=F32
    ).astype(BF)
    back = jnp.concatenate(
        [expert_out.reshape(n_ep, cap, quarter), dense_out.reshape(n_ep, per_near, quarter)], axis=1
    )
    returned = exchange(back, EP)

    slots = returned[:, :cap].reshape(n_ep * cap, quarter)
    per_choice = dot32(fetch, slots)
    moe = per_choice[:rows] * first_weight + per_choice[rows:] * second_weight
    sides = [lax.axis_size(axis) for axis in EP]
    branch = jnp.sum(
        returned[:, cap:].astype(F32).reshape(*sides, per_near, quarter), axis=(0, 2)
    ).reshape(rows, quarter)
    return (resid_own + moe + branch_weight * branch).astype(BF)


def solution(mesh):
    torus = Mesh(mesh.devices.reshape(4, 2, 4, 2, 2, mesh.shape["tp"]), (*EP, "x"))
    placed = (
        P(EP, None),
        P(EP, "x", None, None),
        P(),
        P(None, "x"),
        P(None, "x"),
        P(None, "x"),
        P(None, "x"),
        P(None, "x"),
        P("x"),
        P(),
        P("x", None),
        P(),
        P(EP, None),
        P(EP),
        P(EP, None),
        P(EP, None, "x"),
        P(EP, None, "x"),
        P(EP, "x", None),
        P(EP, "x"),
        P(EP, "x"),
        P(EP, "x"),
        P(),
    )
    return jax.shard_map(local, mesh=torus, in_specs=placed, out_specs=P(EP, "x"), check_vma=False)
```

```python
import functools

import jax
import jax.numpy as jnp
from jax import lax
from jax.experimental import pallas as pl
from jax.experimental.pallas import tpu as pltpu
from jax.sharding import Mesh
from jax.sharding import PartitionSpec as P

EP = ("z_hi", "z_lo", "y_hi", "y_lo", "c")
NEAR = ("z_lo", "y_lo", "c")
BF = jnp.bfloat16
F32 = jnp.float32


def rms_scale(values, gain, floor):
    return values * lax.rsqrt(jnp.mean(values * values, axis=-1, keepdims=True) + floor) * gain


def unit_rows(values):
    return values * lax.rsqrt(jnp.sum(values * values, axis=-1, keepdims=True) + 1.0)


def dot32(a, b):
    return jnp.dot(a, b, preferred_element_type=F32)


def slots_of(ids_ref, pick_ref, fetch_ref, near, rows):
    choices = ids_ref.shape[0]
    row_ids = ids_ref[...].astype(F32)
    r_at = lax.broadcasted_iota(jnp.int32, (rows, rows), 0)
    c_at = lax.broadcasted_iota(jnp.int32, (rows, rows), 1)
    eye = jnp.where(r_at == c_at, 1.0, 0.0)
    col_ids = lax.dot_general(eye, row_ids, (((1,), (1,)), ((), ())), preferred_element_type=F32)
    row_slots, col_slots = [], []
    for j in range(choices):
        by_row = jnp.zeros((rows, rows), F32)
        by_col = jnp.zeros((rows, rows), F32)
        for o in range(choices):
            by_row += jnp.where(col_ids[:, o : o + 1] == row_ids[j : j + 1, :], 1.0, 0.0)
            by_col += jnp.where(col_ids[:, j : j + 1] == row_ids[o : o + 1, :], 1.0, 0.0)
        row_rank = jnp.sum(jnp.where(r_at < c_at, by_row, 0.0), axis=0, keepdims=True)
        col_rank = jnp.sum(jnp.where(c_at < r_at, by_col, 0.0), axis=1, keepdims=True)
        row_slots.append(row_ids[j : j + 1, :] * 2.0 + row_rank)
        col_slots.append(col_ids[:, j : j + 1] * 2.0 + col_rank)
    place = lax.broadcasted_iota(jnp.int32, (rows, fetch_ref.shape[1]), 1).astype(F32)
    fetch_ref[...] = jnp.concatenate(
        [jnp.where(place == found, 1.0, 0.0) for found in col_slots], axis=0
    ).astype(BF)

    shape = (8, 2 * rows)
    at = lax.broadcasted_iota(jnp.int32, shape, 0)
    col = lax.broadcasted_iota(jnp.int32, shape, 1)
    slot = (at & 1).astype(F32)
    same_half = (at >= 4) == (col >= rows)
    for_expert = (at & 2) == 0
    token = jnp.where(col >= rows, col - rows, col).astype(F32)
    expert_keys = [
        jnp.where(
            same_half & for_expert, jnp.concatenate([found, found], axis=1) - slot, -1.0
        )
        for found in row_slots
    ]
    dense_key = jnp.where(same_half, jnp.where(for_expert, -1.0, token - slot), -1.0)
    dense_hit = [dense_key == 2.0 * n for n in range(near)]
    blocks = []
    for d in range(pick_ref.shape[0] // 8):
        hit = dense_hit[d // 16 % 2 * 4 + d // 2 % 2 * 2 + d % 2]
        for key in expert_keys:
            hit = hit | (key == 2.0 * d)
        blocks.append(jnp.where(hit, 1.0, 0.0))
    pick_ref[...] = jnp.concatenate(blocks, axis=0).astype(BF)


def mixer_body(near, *refs):
    rate_ref, sources, targets, buffers = refs[0], refs[1:12], refs[12:15], refs[15:26]
    sems = refs[26]
    partial_ref, pick_ref, fetch_ref = targets
    (
        hidden_ref,
        gain_ref,
        decay_ref,
        beta_ref,
        head_gain_ref,
        ids_ref,
        query_ref,
        key_ref,
        value_ref,
        out_w_ref,
        state_ref,
    ) = buffers
    rows = hidden_ref.shape[0]
    heads = decay_ref.shape[0]
    dv = head_gain_ref.shape[1]
    dk = query_ref.shape[1] // heads
    groups = 4
    step = state_ref.shape[0] // groups

    def copy_of(source, target, at):
        return pltpu.make_async_copy(source, target, sems.at[at])

    gets = [copy_of(sources[n], buffers[n], n) for n in range(10)]
    get_state = [
        copy_of(
            sources[10].at[pl.ds(g * step, step)], state_ref.at[pl.ds(g * step, step)], 10 + g
        )
        for g in range(groups)
    ]
    for copy in gets[:8] + get_state + gets[8:]:
        copy.start()
    gets[5].wait()
    slots_of(ids_ref, pick_ref, fetch_ref, near, rows)
    for copy in gets[:5]:
        copy.wait()
    wide = hidden_ref[...].astype(F32)
    normed = rms_scale(wide, gain_ref[...], 0.1).astype(BF)
    wide = normed.astype(F32)
    gets[6].wait()
    q_all = dot32(normed, query_ref[...])
    gets[7].wait()
    k_all = dot32(normed, key_ref[...])
    units = []
    for source in (q_all, k_all):
        for h in range(heads):
            units.append(unit_rows(source[:, h * dk : (h + 1) * dk]))
    stacked = jnp.concatenate(units, axis=0).astype(BF)
    pairs = heads * rows
    row_at = lax.broadcasted_iota(jnp.int32, stacked.shape, 0) % pairs
    zero = jnp.zeros_like(stacked)
    read = jnp.zeros((2 * pairs, dv), F32)
    for g in range(groups):
        get_state[g].wait()
        blocks = []
        for b in range(g * step // dk, (g + 1) * step // dk):
            blocks.append(jnp.where(row_at == (b % heads) * rows + b // heads, stacked, zero))
        state = state_ref[g * step : (g + 1) * step].astype(BF)
        read = read + dot32(jnp.concatenate(blocks, axis=1), state)
    gets[8].wait()
    v_all = dot32(normed, value_ref[...])
    outs = []
    for h in range(heads):
        lanes = slice(h * dv, (h + 1) * dv)
        decay_in = jnp.sum(wide * decay_ref[h : h + 1, :].astype(F32), axis=1, keepdims=True)
        beta_in = jnp.sum(wide * beta_ref[h : h + 1, :].astype(F32), axis=1, keepdims=True)
        decay = jnp.exp(-rate_ref[h] * jax.nn.softplus(decay_in))
        meet = jnp.sum(units[h] * units[heads + h], axis=1, keepdims=True)
        meet = meet * jax.nn.sigmoid(beta_in)
        read_q = read[h * rows : (h + 1) * rows]
        read_k = read[pairs + h * rows : pairs + (h + 1) * rows]
        readout = decay * read_q + meet * (v_all[:, lanes] - decay * read_k)
        outs.append(rms_scale(readout, head_gain_ref[...], 0.01).astype(BF))
    head_out = jnp.concatenate(outs, axis=1)
    gets[9].wait()
    partial = dot32(head_out, out_w_ref[...]).astype(BF)
    for t in range(partial_ref.shape[0]):
        partial_ref[t] = partial


def mixer(hidden, state, gain, query, key, value, decay, beta, rate, head_gain, out_w, ids, n_ep, n_tp, near):
    rows, width = hidden.shape
    smem = pl.BlockSpec(memory_space=pltpu.SMEM)
    anywhere = pl.BlockSpec(memory_space=pl.ANY)
    arrays = (
        hidden,
        gain[None],
        decay.T,
        beta.T,
        head_gain[None],
        ids.T,
        query,
        key,
        value,
        out_w,
        state.reshape(-1, state.shape[-1]),
    )
    outs = (
        pltpu.VMEM((n_tp, rows, width), BF),
        pltpu.VMEM((n_ep * 8, 2 * rows), BF),
        pltpu.VMEM((ids.size, 2 * n_ep), BF),
    )
    return pl.pallas_call(
        functools.partial(mixer_body, near),
        out_shape=outs,
        in_specs=[smem] + [anywhere] * len(arrays),
        out_specs=(pl.BlockSpec(memory_space=pltpu.VMEM),) * len(outs),
        scratch_shapes=[pltpu.VMEM(a.shape, a.dtype) for a in arrays]
        + [pltpu.SemaphoreType.DMA((14,))],
        name="mixer",
    )(rate, *arrays)


def spread_body(*refs):
    sources, target = refs[:-1], refs[-1]
    rows = sources[0].shape[0]
    for w, source in enumerate(sources):
        for c in range(target.shape[0]):
            target[c, w * rows : (w + 1) * rows, :] = source[...]


def spread(weights, count):
    rows, width = weights[0].shape
    vmem = pl.BlockSpec(memory_space=pltpu.VMEM)
    return pl.pallas_call(
        spread_body,
        out_shape=jax.ShapeDtypeStruct((count, len(weights) * rows, width), BF),
        in_specs=[vmem] * len(weights),
        out_specs=vmem,
        name="spread",
    )(*weights)


def exchange(blocks, axis):
    return lax.all_to_all(blocks, axis, split_axis=0, concat_axis=0, tiled=True)


def local(
    hidden_in,
    prior_state,
    mix_gain,
    query_w,
    key_w,
    value_w,
    decay_w,
    beta_w,
    decay_rate,
    head_gain,
    out_w,
    ffn_gain,
    expert_ids,
    group_share,
    expert_share,
    expert_gate,
    expert_up,
    expert_down,
    dense_gate,
    dense_up,
    dense_down,
    branch_gate,
):
    rows, width = hidden_in.shape
    n_ep = lax.axis_size(EP)
    n_tp = lax.axis_size("x")
    n_near = lax.axis_size(NEAR)
    quarter = width // n_tp
    cap = 2
    per_near = rows // n_near
    tp_at = lax.axis_index("x")
    hid = dense_gate.shape[0]

    copies = spread((dense_gate, dense_up, dense_down), n_near)
    dense_near = exchange(copies, NEAR).reshape(n_near, 3, hid, quarter)

    copies_out, pick, fetch = mixer(
        hidden_in,
        prior_state,
        mix_gain,
        query_w,
        key_w,
        value_w,
        decay_w,
        beta_w,
        decay_rate,
        head_gain,
        out_w,
        expert_ids,
        n_ep,
        n_tp,
        n_near,
    )
    fetch, group_share, expert_share, branch_gate, tp_at = lax.optimization_barrier(
        (fetch, group_share, expert_share, branch_gate, tp_at)
    )
    fetch, expert_gate, expert_up, expert_down = lax.optimization_barrier(
        (fetch, expert_gate, expert_up, expert_down)
    )
    n_hid = n_near * hid
    share = n_hid // n_tp
    pairs_near = dense_near[:, :2].reshape(n_tp, -1, 2, hid, quarter)
    both_near = jnp.swapaxes(pairs_near, 1, 2).reshape(2 * n_hid, quarter)
    down_near = dense_near[:, 2].reshape(n_hid, quarter)
    expert_both = jnp.concatenate([expert_gate[0], expert_up[0]], axis=1)
    down_blocks = [expert_down[0, :, t * quarter : (t + 1) * quarter] for t in range(n_tp)]
    packed = jnp.concatenate([expert_both, *down_blocks], axis=0)
    swap = [(t, t ^ 1) for t in range(n_tp)]
    from_partner = lax.ppermute(packed, "x", swap)
    route_weight = (
        group_share[:, None] * expert_share / jnp.sum(expert_share, axis=1, keepdims=True)
    )
    first_weight, second_weight = route_weight[:, :1], route_weight[:, 1:]
    gate_wide = branch_gate.astype(F32)
    half = quarter // 2
    offset, offset_half = tp_at * quarter, tp_at * quarter + half
    copies_out, both_near, down_near, fetch, offset, offset_half = lax.optimization_barrier(
        (copies_out, both_near, down_near, fetch, offset, offset_half)
    )
    copies_out, expert_both, first_weight, second_weight, gate_wide = lax.optimization_barrier(
        (copies_out, expert_both, first_weight, second_weight, gate_wide)
    )
    partials = exchange(copies_out, "x")
    mix = jnp.sum(partials.astype(F32), axis=0)
    resid = (hidden_in.astype(F32) + mix).astype(BF)
    normed2 = rms_scale(resid.astype(F32), ffn_gain, 0.1).astype(BF)
    resid_own = lax.dynamic_slice_in_dim(
        resid, offset, quarter, 1, allow_negative_indices=False
    ).astype(F32)
    branch_dot = jnp.sum(normed2.astype(F32) * gate_wide, axis=1, keepdims=True)
    branch_weight = jax.nn.sigmoid(branch_dot)

    block = cap + per_near
    halves = jnp.concatenate(
        [
            lax.dynamic_slice_in_dim(normed2, start, half, 1, allow_negative_indices=False)
            for start in (offset, offset_half)
        ],
        axis=0,
    )
    sent = dot32(pick, halves).astype(BF)
    sent, branch_weight, resid_own = lax.optimization_barrier((sent, branch_weight, resid_own))
    arrived = exchange(sent.reshape(n_ep, 8, quarter // 2), EP)
    arrived = arrived.reshape(n_ep, 2, block, quarter // 2)
    arrived = jnp.concatenate([arrived[:, 0], arrived[:, 1]], axis=2)
    moe_rows = arrived[:, :cap].reshape(n_ep * cap, quarter)
    dense_rows = arrived[:, cap:].reshape(n_ep * per_near, quarter)

    contract = (((1,), (1,)), ((), ()))
    pre = lax.dot_general(both_near, dense_rows, contract, preferred_element_type=F32)
    pre = pre.astype(BF)
    pre = pre.reshape(n_tp, 2 * share, -1)
    served = n_ep * cap // 2
    moe_halves = jnp.concatenate([moe_rows] * (n_tp // 2), axis=0).reshape(n_tp, served, quarter)
    partner_both = from_partner[:width]
    units = expert_down.shape[1]
    partner_down = jnp.concatenate(
        [from_partner[width + t * units : width + (t + 1) * units] for t in range(n_tp)], axis=1
    )
    first = jnp.concatenate([moe_halves, pre], axis=1)
    first, partner_both, partner_down = lax.optimization_barrier(
        (first, partner_both, partner_down)
    )
    first = exchange(first, "x")

    pre_sum = jnp.sum(first[:, served:].astype(F32), axis=0)
    dense_hidden = (jax.nn.silu(pre_sum[:share]) * pre_sum[share:]).astype(BF)
    full_rows = jnp.concatenate([first[t, :served] for t in range(n_tp)], axis=1)
    expert_part = 0.0
    for w_both, w_down in ((expert_both, expert_down[0]), (partner_both, partner_down)):
        both_pre = dot32(full_rows, w_both)
        hidden = (jax.nn.silu(both_pre[:, :units]) * both_pre[:, units:]).astype(BF)
        expert_part = expert_part + dot32(hidden, w_down)
    expert_part = expert_part.astype(BF)
    part_blocks = jnp.stack(
        [expert_part[:, t * quarter : (t + 1) * quarter] for t in range(n_tp)], axis=0
    )
    hidden_copies = jnp.broadcast_to(dense_hidden, (n_tp, *dense_hidden.shape))
    second = exchange(jnp.concatenate([part_blocks, hidden_copies], axis=1), "x")

    by_pair = second[:, :served].astype(F32).reshape(n_tp // 2, 2 * served, quarter)
    expert_out = jnp.sum(by_pair, axis=0).astype(BF)
    all_hidden = second[:, served:].reshape(n_hid, -1)
    dense_out = lax.dot_general(
        all_hidden, down_near, (((0,), (0,)), ((), ())), preferred_element_type=F32
    ).astype(BF)
    back = jnp.concatenate(
        [expert_out.reshape(n_ep, cap, quarter), dense_out.reshape(n_ep, per_near, quarter)], axis=1
    )
    returned = exchange(back, EP)

    slots = returned[:, :cap].reshape(n_ep * cap, quarter)
    per_choice = dot32(fetch, slots)
    moe = per_choice[:rows] * first_weight + per_choice[rows:] * second_weight
    sides = [lax.axis_size(axis) for axis in EP]
    branch = jnp.sum(
        returned[:, cap:].astype(F32).reshape(*sides, per_near, quarter), axis=(0, 2)
    ).reshape(rows, quarter)
    return (resid_own + moe + branch_weight * branch).astype(BF)


def solution(mesh):
    torus = Mesh(mesh.devices.reshape(4, 2, 4, 2, 2, mesh.shape["tp"]), (*EP, "x"))
    placed = (
        P(EP, None),
        P(EP, "x", None, None),
        P(),
        P(None, "x"),
        P(None, "x"),
        P(None, "x"),
        P(None, "x"),
        P(None, "x"),
        P("x"),
        P(),
        P("x", None),
        P(),
        P(EP, None),
        P(EP),
        P(EP, None),
        P(EP, None, "x"),
        P(EP, None, "x"),
        P(EP, "x", None),
        P(EP, "x"),
        P(EP, "x"),
        P(EP, "x"),
        P(),
    )
    return jax.shard_map(local, mesh=torus, in_specs=placed, out_specs=P(EP, "x"), check_vma=False)
```

```python
import functools

import jax
import jax.numpy as jnp
from jax import lax
from jax.experimental import pallas as pl
from jax.experimental.pallas import tpu as pltpu
from jax.sharding import Mesh
from jax.sharding import PartitionSpec as P

EP = ("z_hi", "z_lo", "y_hi", "y_lo", "c")
NEAR = ("z_lo", "y_lo", "c")
BF = jnp.bfloat16
F32 = jnp.float32


def rms_scale(values, gain, floor):
    return values * lax.rsqrt(jnp.mean(values * values, axis=-1, keepdims=True) + floor) * gain


def unit_rows(values):
    return values * lax.rsqrt(jnp.sum(values * values, axis=-1, keepdims=True) + 1.0)


def dot32(a, b):
    return jnp.dot(a, b, preferred_element_type=F32)


def slots_of(ids_ref, pick_ref, fetch_ref, near, rows):
    choices = ids_ref.shape[0]
    row_ids = ids_ref[...].astype(F32)
    r_at = lax.broadcasted_iota(jnp.int32, (rows, rows), 0)
    c_at = lax.broadcasted_iota(jnp.int32, (rows, rows), 1)
    eye = jnp.where(r_at == c_at, 1.0, 0.0)
    col_ids = lax.dot_general(eye, row_ids, (((1,), (1,)), ((), ())), preferred_element_type=F32)
    row_slots, col_slots = [], []
    for j in range(choices):
        by_row = jnp.zeros((rows, rows), F32)
        by_col = jnp.zeros((rows, rows), F32)
        for o in range(choices):
            by_row += jnp.where(col_ids[:, o : o + 1] == row_ids[j : j + 1, :], 1.0, 0.0)
            by_col += jnp.where(col_ids[:, j : j + 1] == row_ids[o : o + 1, :], 1.0, 0.0)
        row_rank = jnp.sum(jnp.where(r_at < c_at, by_row, 0.0), axis=0, keepdims=True)
        col_rank = jnp.sum(jnp.where(c_at < r_at, by_col, 0.0), axis=1, keepdims=True)
        row_slots.append(row_ids[j : j + 1, :] * 2.0 + row_rank)
        col_slots.append(col_ids[:, j : j + 1] * 2.0 + col_rank)
    place = lax.broadcasted_iota(jnp.int32, (rows, fetch_ref.shape[1]), 1).astype(F32)
    fetch_ref[...] = jnp.concatenate(
        [jnp.where(place == found, 1.0, 0.0) for found in col_slots], axis=0
    ).astype(BF)

    shape = (8, 2 * rows)
    at = lax.broadcasted_iota(jnp.int32, shape, 0)
    col = lax.broadcasted_iota(jnp.int32, shape, 1)
    slot = (at & 1).astype(F32)
    same_half = (at >= 4) == (col >= rows)
    for_expert = (at & 2) == 0
    token = jnp.where(col >= rows, col - rows, col).astype(F32)
    expert_keys = [
        jnp.where(
            same_half & for_expert, jnp.concatenate([found, found], axis=1) - slot, -1.0
        )
        for found in row_slots
    ]
    dense_key = jnp.where(same_half, jnp.where(for_expert, -1.0, token - slot), -1.0)
    dense_hit = [dense_key == 2.0 * n for n in range(near)]
    blocks = []
    for d in range(pick_ref.shape[0] // 8):
        hit = dense_hit[d // 16 % 2 * 4 + d // 2 % 2 * 2 + d % 2]
        for key in expert_keys:
            hit = hit | (key == 2.0 * d)
        blocks.append(jnp.where(hit, 1.0, 0.0))
    pick_ref[...] = jnp.concatenate(blocks, axis=0).astype(BF)


def mixer_body(near, *refs):
    rate_ref, sources, targets, buffers = refs[0], refs[1:12], refs[12:15], refs[15:26]
    sems = refs[26]
    partial_ref, pick_ref, fetch_ref = targets
    (
        hidden_ref,
        gain_ref,
        decay_ref,
        beta_ref,
        head_gain_ref,
        ids_ref,
        query_ref,
        key_ref,
        value_ref,
        out_w_ref,
        state_ref,
    ) = buffers
    rows = hidden_ref.shape[0]
    heads = decay_ref.shape[0]
    dv = head_gain_ref.shape[1]
    dk = query_ref.shape[1] // heads
    groups = 4
    step = state_ref.shape[0] // groups

    def copy_of(source, target, at):
        return pltpu.make_async_copy(source, target, sems.at[at])

    gets = [copy_of(sources[n], buffers[n], n) for n in range(10)]
    get_state = [
        copy_of(
            sources[10].at[pl.ds(g * step, step)], state_ref.at[pl.ds(g * step, step)], 10 + g
        )
        for g in range(groups)
    ]
    for copy in gets[:8] + get_state + gets[8:]:
        copy.start()
    gets[5].wait()
    slots_of(ids_ref, pick_ref, fetch_ref, near, rows)
    for copy in gets[:5]:
        copy.wait()
    wide = hidden_ref[...].astype(F32)
    normed = rms_scale(wide, gain_ref[...], 0.1).astype(BF)
    wide = normed.astype(F32)
    gets[6].wait()
    q_all = dot32(normed, query_ref[...])
    gets[7].wait()
    k_all = dot32(normed, key_ref[...])
    units = []
    for source in (q_all, k_all):
        for h in range(heads):
            units.append(unit_rows(source[:, h * dk : (h + 1) * dk]))
    stacked = jnp.concatenate(units, axis=0).astype(BF)
    pairs = heads * rows
    row_at = lax.broadcasted_iota(jnp.int32, stacked.shape, 0) % pairs
    zero = jnp.zeros_like(stacked)
    read = jnp.zeros((2 * pairs, dv), F32)
    for g in range(groups):
        get_state[g].wait()
        blocks = []
        for b in range(g * step // dk, (g + 1) * step // dk):
            blocks.append(jnp.where(row_at == (b % heads) * rows + b // heads, stacked, zero))
        state = state_ref[g * step : (g + 1) * step].astype(BF)
        read = read + dot32(jnp.concatenate(blocks, axis=1), state)
    gets[8].wait()
    v_all = dot32(normed, value_ref[...])
    outs = []
    for h in range(heads):
        lanes = slice(h * dv, (h + 1) * dv)
        decay_in = jnp.sum(wide * decay_ref[h : h + 1, :].astype(F32), axis=1, keepdims=True)
        beta_in = jnp.sum(wide * beta_ref[h : h + 1, :].astype(F32), axis=1, keepdims=True)
        decay = jnp.exp(-rate_ref[h] * jax.nn.softplus(decay_in))
        meet = jnp.sum(units[h] * units[heads + h], axis=1, keepdims=True)
        meet = meet * jax.nn.sigmoid(beta_in)
        read_q = read[h * rows : (h + 1) * rows]
        read_k = read[pairs + h * rows : pairs + (h + 1) * rows]
        readout = decay * read_q + meet * (v_all[:, lanes] - decay * read_k)
        outs.append(rms_scale(readout, head_gain_ref[...], 0.01).astype(BF))
    head_out = jnp.concatenate(outs, axis=1)
    gets[9].wait()
    partial = dot32(head_out, out_w_ref[...]).astype(BF)
    for t in range(partial_ref.shape[0]):
        partial_ref[t] = partial


def mixer(hidden, state, gain, query, key, value, decay, beta, rate, head_gain, out_w, ids, n_ep, n_tp, near):
    rows, width = hidden.shape
    smem = pl.BlockSpec(memory_space=pltpu.SMEM)
    anywhere = pl.BlockSpec(memory_space=pl.ANY)
    arrays = (
        hidden,
        gain[None],
        decay.T,
        beta.T,
        head_gain[None],
        ids.T,
        query,
        key,
        value,
        out_w,
        state.reshape(-1, state.shape[-1]),
    )
    outs = (
        pltpu.VMEM((n_tp, rows, width), BF),
        pltpu.VMEM((n_ep * 8, 2 * rows), BF),
        pltpu.VMEM((ids.size, 2 * n_ep), BF),
    )
    return pl.pallas_call(
        functools.partial(mixer_body, near),
        out_shape=outs,
        in_specs=[smem] + [anywhere] * len(arrays),
        out_specs=(pl.BlockSpec(memory_space=pltpu.VMEM),) * len(outs),
        scratch_shapes=[pltpu.VMEM(a.shape, a.dtype) for a in arrays]
        + [pltpu.SemaphoreType.DMA((14,))],
        name="mixer",
    )(rate, *arrays)


def spread_body(*refs):
    sources, target = refs[:-1], refs[-1]
    rows = sources[0].shape[0]
    for w, source in enumerate(sources):
        for c in range(target.shape[0]):
            target[c, w * rows : (w + 1) * rows, :] = source[...]


def spread(weights, count):
    rows, width = weights[0].shape
    vmem = pl.BlockSpec(memory_space=pltpu.VMEM)
    return pl.pallas_call(
        spread_body,
        out_shape=jax.ShapeDtypeStruct((count, len(weights) * rows, width), BF),
        in_specs=[vmem] * len(weights),
        out_specs=vmem,
        name="spread",
    )(*weights)


def exchange(blocks, axis):
    return lax.all_to_all(blocks, axis, split_axis=0, concat_axis=0, tiled=True)


def local(
    hidden_in,
    prior_state,
    mix_gain,
    query_w,
    key_w,
    value_w,
    decay_w,
    beta_w,
    decay_rate,
    head_gain,
    out_w,
    ffn_gain,
    expert_ids,
    group_share,
    expert_share,
    expert_gate,
    expert_up,
    expert_down,
    dense_gate,
    dense_up,
    dense_down,
    branch_gate,
):
    rows, width = hidden_in.shape
    n_ep = lax.axis_size(EP)
    n_tp = lax.axis_size("x")
    n_near = lax.axis_size(NEAR)
    quarter = width // n_tp
    cap = 2
    per_near = rows // n_near
    tp_at = lax.axis_index("x")
    hid = dense_gate.shape[0]

    copies = spread((dense_gate, dense_up, dense_down), n_near)
    dense_near = exchange(copies, NEAR).reshape(n_near, 3, hid, quarter)

    copies_out, pick, fetch = mixer(
        hidden_in,
        prior_state,
        mix_gain,
        query_w,
        key_w,
        value_w,
        decay_w,
        beta_w,
        decay_rate,
        head_gain,
        out_w,
        expert_ids,
        n_ep,
        n_tp,
        n_near,
    )
    fetch, group_share, expert_share, branch_gate, tp_at = lax.optimization_barrier(
        (fetch, group_share, expert_share, branch_gate, tp_at)
    )
    fetch, expert_gate, expert_up, expert_down = lax.optimization_barrier(
        (fetch, expert_gate, expert_up, expert_down)
    )
    n_hid = n_near * hid
    share = n_hid // n_tp
    pairs_near = dense_near[:, :2].reshape(n_tp, -1, 2, hid, quarter)
    both_near = jnp.swapaxes(pairs_near, 1, 2).reshape(2 * n_hid, quarter)
    down_near = dense_near[:, 2].reshape(n_hid, quarter)
    expert_both = jnp.concatenate([expert_gate[0], expert_up[0]], axis=1)
    down_blocks = [expert_down[0, :, t * quarter : (t + 1) * quarter] for t in range(n_tp)]
    packed = jnp.concatenate([expert_both, *down_blocks], axis=0)
    swap = [(t, t ^ 1) for t in range(n_tp)]
    from_partner = lax.ppermute(packed, "x", swap)
    route_weight = (
        group_share[:, None] * expert_share / jnp.sum(expert_share, axis=1, keepdims=True)
    )
    first_weight, second_weight = route_weight[:, :1], route_weight[:, 1:]
    gate_wide = branch_gate.astype(F32)
    half = quarter // 2
    offset, offset_half = tp_at * quarter, tp_at * quarter + half
    copies_out, both_near, down_near, fetch, offset, offset_half = lax.optimization_barrier(
        (copies_out, both_near, down_near, fetch, offset, offset_half)
    )
    copies_out, expert_both, first_weight, second_weight, gate_wide = lax.optimization_barrier(
        (copies_out, expert_both, first_weight, second_weight, gate_wide)
    )
    partials = exchange(copies_out, "x")
    mix = jnp.sum(partials.astype(F32), axis=0)
    resid = (hidden_in.astype(F32) + mix).astype(BF)
    normed2 = rms_scale(resid.astype(F32), ffn_gain, 0.1).astype(BF)
    resid_own = lax.dynamic_slice_in_dim(
        resid, offset, quarter, 1, allow_negative_indices=False
    ).astype(F32)
    branch_dot = jnp.sum(normed2.astype(F32) * gate_wide, axis=1, keepdims=True)
    branch_weight = jax.nn.sigmoid(branch_dot)

    block = cap + per_near
    halves = jnp.concatenate(
        [
            lax.dynamic_slice_in_dim(normed2, start, half, 1, allow_negative_indices=False)
            for start in (offset, offset_half)
        ],
        axis=0,
    )
    sent = dot32(pick, halves).astype(BF)
    sent, branch_weight, resid_own = lax.optimization_barrier((sent, branch_weight, resid_own))
    arrived = exchange(sent.reshape(n_ep, 8, quarter // 2), EP)
    arrived = arrived.reshape(n_ep, 2, block, quarter // 2)
    arrived = jnp.concatenate([arrived[:, 0], arrived[:, 1]], axis=2)
    moe_rows = arrived[:, :cap].reshape(n_ep * cap, quarter)
    dense_rows = arrived[:, cap:].reshape(n_ep * per_near, quarter)

    contract = (((1,), (1,)), ((), ()))
    pre = lax.dot_general(both_near, dense_rows, contract, preferred_element_type=F32)
    pre = pre.astype(BF)
    pre = pre.reshape(n_tp, 2 * share, -1)
    served = n_ep * cap // 2
    moe_halves = jnp.concatenate([moe_rows] * (n_tp // 2), axis=0).reshape(n_tp, served, quarter)
    partner_both = from_partner[:width]
    units = expert_down.shape[1]
    partner_down = jnp.concatenate(
        [from_partner[width + t * units : width + (t + 1) * units] for t in range(n_tp)], axis=1
    )
    first = jnp.concatenate([moe_halves, pre], axis=1)
    w_both = jnp.concatenate([expert_both, partner_both], axis=1)
    w_down = jnp.concatenate([expert_down[0], partner_down], axis=0)
    first, w_both, w_down = lax.optimization_barrier((first, w_both, w_down))
    first = exchange(first, "x")

    pre_sum = jnp.sum(first[:, served:].astype(F32), axis=0)
    dense_hidden = (jax.nn.silu(pre_sum[:share]) * pre_sum[share:]).astype(BF)
    full_rows = jnp.concatenate([first[t, :served] for t in range(n_tp)], axis=1)
    both_pre = dot32(full_rows, w_both)
    gates = [both_pre[:, n * units : (n + 1) * units] for n in range(4)]
    hidden = jnp.concatenate(
        [jax.nn.silu(gates[0]) * gates[1], jax.nn.silu(gates[2]) * gates[3]], axis=1
    ).astype(BF)
    expert_part = dot32(hidden, w_down).astype(BF)
    part_blocks = jnp.stack(
        [expert_part[:, t * quarter : (t + 1) * quarter] for t in range(n_tp)], axis=0
    )
    hidden_copies = jnp.broadcast_to(dense_hidden, (n_tp, *dense_hidden.shape))
    second = exchange(jnp.concatenate([part_blocks, hidden_copies], axis=1), "x")

    by_pair = second[:, :served].astype(F32).reshape(n_tp // 2, 2 * served, quarter)
    expert_out = jnp.sum(by_pair, axis=0).astype(BF)
    all_hidden = second[:, served:].reshape(n_hid, -1)
    dense_out = lax.dot_general(
        all_hidden, down_near, (((0,), (0,)), ((), ())), preferred_element_type=F32
    ).astype(BF)
    back = jnp.concatenate(
        [expert_out.reshape(n_ep, cap, quarter), dense_out.reshape(n_ep, per_near, quarter)], axis=1
    )
    returned = exchange(back, EP)

    slots = returned[:, :cap].reshape(n_ep * cap, quarter)
    per_choice = dot32(fetch, slots)
    moe = per_choice[:rows] * first_weight + per_choice[rows:] * second_weight
    sides = [lax.axis_size(axis) for axis in EP]
    branch = jnp.sum(
        returned[:, cap:].astype(F32).reshape(*sides, per_near, quarter), axis=(0, 2)
    ).reshape(rows, quarter)
    return (resid_own + moe + branch_weight * branch).astype(BF)


def solution(mesh):
    torus = Mesh(mesh.devices.reshape(4, 2, 4, 2, 2, mesh.shape["tp"]), (*EP, "x"))
    placed = (
        P(EP, None),
        P(EP, "x", None, None),
        P(),
        P(None, "x"),
        P(None, "x"),
        P(None, "x"),
        P(None, "x"),
        P(None, "x"),
        P("x"),
        P(),
        P("x", None),
        P(),
        P(EP, None),
        P(EP),
        P(EP, None),
        P(EP, None, "x"),
        P(EP, None, "x"),
        P(EP, "x", None),
        P(EP, "x"),
        P(EP, "x"),
        P(EP, "x"),
        P(),
    )
    return jax.shard_map(local, mesh=torus, in_specs=placed, out_specs=P(EP, "x"), check_vma=False)
```
